256 devices in a mesh: gr: 2 (over z_hi), fs: 16 (over z_lo, x), tp: 8 (over y, core).
Axes of the slice: x: 4, y: 4, z: 8 (z_hi: 2, z_lo: 4; z = z_hi * 4 + z_lo), core: 2. Of those that a mesh axis runs over, the one named last changes fastest.
Arguments:
- tokens: bfloat16 [6144, 4096], P(('gr', 'fs'), 'tp'), may hold values from -6 to 6
- route_ids: int32 [6144, 2], P(('gr', 'fs')), may hold values from 0 to 15, all different within a row; in each aligned block of 192 rows (0 to 191, 192 to 383, ...) at most 48 rows name the same one
- route_logits: float32 [6144, 2], P(('gr', 'fs')), may hold values from -6 to 6
- gain: float32 [4096], P(('gr', 'fs')), may hold values from 0.1 to 1.9
- gate_master: float32 [16, 4096, 2048], P(None, ('gr', 'fs'), 'tp'), may hold values from -6 to 6
- up_master: float32 [16, 4096, 2048], P(None, ('gr', 'fs'), 'tp'), may hold values from -6 to 6
- down_master: float32 [16, 2048, 4096], P(None, ('gr', 'fs'), 'tp'), may hold values from -6 to 6
Outputs:
- gate_weight: bfloat16 [16, 4096, 2048], P('fs', None, 'tp')
- up_weight: bfloat16 [16, 4096, 2048], P('fs', None, 'tp')
- down_weight: bfloat16 [16, 2048, 4096], P('fs', 'tp')
- mixed_out: bfloat16 [6144, 4096], P(('gr', 'fs'), 'tp')
The draws below stay inside these ranges and needn't reach their ends.
Inputs may be any that keep to these rules, and one draw needn't show every extreme that they name: `route_ids`: each row names 2 different experts; among the rows of one device no expert is named by more than 48 rows, a bound that some block reaches.
All inputs are finite; a program needn't handle non-finite values.
Results may differ from the reference program's by a relative error of at most 0.015.
Values may be sent and summed in bfloat16 or wider, within the bound.
A program may use at most 128 MiB of HBM per device.

```python
import math
import jax
import jax.numpy as jnp
import numpy as np
from jax import lax

D = 4096
FF = 2048
TOP = 2
TOK_DEV = 192
EXPERTS = 16
CAP = 48
TOKENS = 6144
N_GR = 2
N_FS = 16
N_TP = 8


def levels(rng, extent, pieces, low, largest):
    def one(position, shards_of):
        draws = jax.random.uniform(jax.random.fold_in(jax.random.fold_in(rng, 6), position), (shards_of,), jnp.float32, low / len(pieces), largest / len(pieces))
        return jnp.repeat(jnp.exp(draws), extent[position] // shards_of).reshape((-1,) + (1,) * (len(extent) - position - 1))

    level = one(*pieces[0])
    for cut in pieces[1:]:
        level = level * one(*cut)
    return level


def deal_out(key, own, number, rows, number_of, top, most, skew):
    order = jax.random.permutation(key, number_of)
    packed, ordinary = portions_of(number_of, rows * top, most, skew, True), portions_of(number_of, rows * top, most, skew, False)
    places = jnp.arange(number_of)

    def named(tallies, offset_by):
        used = int((tallies > 0).sum())
        fixed = max(1, used // 4)
        passed = fixed + (places - fixed + offset_by * (used - fixed)) % max(1, number_of - fixed)
        return jnp.zeros((number_of,), jnp.int32).at[order[jnp.where(places < fixed, places, passed)]].set(jnp.asarray(tallies, jnp.int32))

    tallies = jnp.where(number % 4 == 0, named(packed, number // 4), named(ordinary, number - number // 4 - 1))
    mixed = jax.random.permutation(jax.random.fold_in(own, 3), number_of)
    source_of, taker = mixed[0:number_of // 2 * 2:2], mixed[1:number_of // 2 * 2:2]
    margin = jnp.minimum(tallies[source_of] - 1, most - tallies[taker]) // 2
    margin = jnp.where((source_of == order[0]) | (taker == order[0]) | (tallies[taker] == 0), 0, jnp.maximum(margin, 0))
    passed = jax.random.randint(jax.random.fold_in(own, 4), (number_of // 2,), 0, 1 << 20) % (margin + 1)
    tallies = tallies.at[source_of].add(-passed).at[taker].add(passed)
    items = jnp.searchsorted(jnp.cumsum(tallies), jnp.arange(rows * top), side="right").astype(jnp.int32)
    table = items.reshape(top, rows).T
    table = table[jax.random.permutation(jax.random.fold_in(own, 1), rows)]
    offset_by = jax.random.randint(jax.random.fold_in(own, 2), (rows, 1), 0, top)
    return jnp.take_along_axis(table, (jnp.arange(top)[None, :] + offset_by) % top, axis=1)


def portions_of(amount, total, bound, skew, full):
    weights = [(1 << 20) // math.isqrt(standing ** skew) + 1 for standing in range(1, amount + 1)]
    largest = bound if full else min(bound, max(-(-total // amount), total * weights[0] // sum(weights)))
    least = 1 if total - largest >= amount - 1 else 0
    given, spare = [largest] + [least] * (amount - 1), total - largest - least * (amount - 1)
    while spare > 0:
        candidates = [i for i in range(1, amount) if given[i] < largest] or [i for i in range(1, amount) if given[i] < bound]
        mass, remaining = sum([weights[i] for i in candidates]), spare
        for i in candidates:
            more = min(bound - given[i], max(1, remaining * weights[i] // mass), spare)
            given[i] = given[i] + more
            spare = spare - more
    return np.array(given)


def bell_draw(key, extent, spread, reach, shards=(), held_as=jnp.bfloat16):
    values = jax.random.normal(key, extent, jnp.float32) * spread
    if len(shards) > 0:
        values = levels(key, extent, shards, -0.22, 0.18) * values
    return jnp.clip(values, min=-reach, max=reach).astype(held_as)


def setup_inputs(seed: int = 0) -> dict:
    seeds = jax.random.split(jax.random.key(seed), 8)
    tokens = bell_draw(seeds[0], (TOKENS, D), 1.0, 6.0, ((0, 32), (1, 8)))
    route_ids_keys = jax.random.split(jax.random.fold_in(seeds[1], 1), TOKENS // TOK_DEV)
    route_ids_turns = jax.random.permutation(jax.random.fold_in(seeds[1], 3), TOKENS // TOK_DEV)
    route_ids = jax.vmap(lambda own, number: deal_out(jax.random.fold_in(seeds[1], 2), own, number, TOK_DEV, EXPERTS, TOP, CAP, 2))(route_ids_keys, route_ids_turns).reshape((TOKENS, TOP))
    route_logits = bell_draw(seeds[2], (TOKENS, TOP), 1.5, 6.0, ((0, 32),), jnp.float32)
    gain = jnp.clip(1.0 + 0.18 * jax.random.normal(seeds[3], (D,), jnp.float32), 0.1, 1.9)
    gate_master = bell_draw(seeds[4], (EXPERTS, D, FF), 1.0, 6.0, ((1, 32), (2, 8)), jnp.float32)
    up_master = bell_draw(seeds[5], (EXPERTS, D, FF), 1.0, 6.0, ((1, 32), (2, 8)), jnp.float32)
    down_master = bell_draw(seeds[6], (EXPERTS, FF, D), 1.0, 6.0, ((1, 32), (2, 8)), jnp.float32)
    return dict(tokens=tokens, route_ids=route_ids, route_logits=route_logits, gain=gain, gate_master=gate_master, up_master=up_master, down_master=down_master)


EPS = 1e-06

def reference(tokens, route_ids, route_logits, gain, gate_master, up_master, down_master):
    row_gain = gain[None, :, None]
    gate_weight = (gate_master * row_gain).astype(jnp.bfloat16)
    up_weight = (up_master * row_gain).astype(jnp.bfloat16)
    down_weight = down_master.astype(jnp.bfloat16)
    float_rows = tokens.astype(jnp.float32)
    normed = (float_rows * lax.rsqrt(lax.optimization_barrier(jnp.mean(float_rows * float_rows, axis=1, keepdims=True)) + EPS)).astype(jnp.bfloat16)
    sigmoid_vals = jax.nn.sigmoid(route_logits.astype(jnp.float32))
    shares = sigmoid_vals / lax.optimization_barrier(jnp.sum(sigmoid_vals, axis=1, keepdims=True))
    assign_count = TOKENS * TOP
    slot_limit = N_GR * N_FS * CAP
    flattened = route_ids.reshape(assign_count).astype(jnp.int32)
    sort_order = jnp.argsort(flattened).astype(jnp.int32)
    starts = jnp.searchsorted(flattened[sort_order], jnp.arange(EXPERTS, dtype=jnp.int32), side='left').astype(jnp.int32)
    padded_order = jnp.concatenate([sort_order, jnp.full((slot_limit,), assign_count, jnp.int32)])
    padded_ids = jnp.concatenate([flattened, jnp.full((1,), -1, jnp.int32)])
    padded_shares = jnp.concatenate([shares.reshape(assign_count), jnp.zeros((1,), jnp.float32)])
    padded_rows = jnp.concatenate([normed, jnp.zeros((1, D), jnp.bfloat16)], axis=0)

    def one_expert(expert):
        picked_index = lax.dynamic_slice_in_dim(padded_order, starts[expert], slot_limit)
        is_valid = padded_ids[picked_index] == expert
        token_index = jnp.where(is_valid, picked_index // TOP, TOKENS).astype(jnp.int32)
        expert_rows = padded_rows[token_index]
        gate_value = jnp.dot(expert_rows, gate_weight[expert], preferred_element_type=jnp.float32) * D ** (-0.5)
        up_value = jnp.dot(expert_rows, up_weight[expert], preferred_element_type=jnp.float32) * D ** (-0.5)
        hidden = (jax.nn.silu(gate_value) * up_value).astype(jnp.bfloat16)
        hidden_blocks = hidden.reshape(slot_limit, N_TP, FF // N_TP).astype(jnp.float32)
        down_blocks = down_weight[expert].reshape(N_TP, FF // N_TP, D).astype(jnp.float32)
        partials = jnp.einsum('mjf,jfd->jmd', hidden_blocks, down_blocks).astype(jnp.bfloat16)
        partials = lax.optimization_barrier(partials)
        expert_out = (lax.optimization_barrier(jnp.sum(partials.astype(jnp.float32), axis=0)) * FF ** (-0.5)).astype(jnp.bfloat16)
        expert_out = lax.optimization_barrier(expert_out)
        weights_here = jnp.where(is_valid, padded_shares[picked_index], jnp.float32(0.0))
        return (token_index, expert_out.astype(jnp.float32) * weights_here[:, None])
    token_lists, terms = lax.map(one_expert, jnp.arange(EXPERTS, dtype=jnp.int32))
    total = jnp.zeros((TOKENS + 1, D), jnp.float32).at[token_lists.reshape(-1)].add(terms.reshape(-1, D))
    mixed_out = total[:TOKENS].astype(jnp.bfloat16)
    return (gate_weight, up_weight, down_weight, mixed_out)
```

```python
import functools

import jax
import jax.numpy as jnp
from jax import lax
from jax.experimental import pallas as pl
from jax.experimental.pallas import tpu as pltpu
from jax.sharding import PartitionSpec as P

EPS = 1e-06
MESH = pl.DeviceIdType.MESH
F32 = jnp.float32
BF16 = jnp.bfloat16
NQ = 4


def kernel(
    dims,
    tok_ref, ids_ref, logit_ref, gain_ref, gate_hbm, up_hbm, down_hbm,
    gate_out, up_out, down_out, mixed_out,
    stage_g, stage_u, stage_d, snd_g, snd_u, snd_d,
    wg, wu, wd, slots, share_hi, share_lo, xall, hidden,
    psend, precv, ysum, yrecv, rsend, rrecv,
    load_sem, disp_s, disp_r, w_s, g_r, u_r, d_r,
    ag_s, ag_r, sib_s, sib_r, ps_s, ps_r, ys_s, ys_r, rt_s, rt_r, out_sem,
):
    n_gr, n_zl, n_x, n_y, n_c, cap = dims
    n_fs = n_zl * n_x
    n_z = n_gr * n_zl
    n_tp = n_y * n_c
    g = lax.axis_index("gr")
    f = lax.axis_index("fs")
    t = lax.axis_index("tp")
    z = g * n_zl + f // n_x
    x = f % n_x
    y = t // n_c
    c = t % n_c
    part = g * n_fs + f
    rows_g = stage_g.shape[1]
    rows_d = stage_d.shape[1]
    wide = tok_ref.shape[1]
    wq = wide // NQ
    n_rows = n_fs * cap
    n_peer = n_z * n_x
    d_model = n_tp * wide
    sibling = (g, f, y * n_c + (1 - c))

    def remote(src, dst, s_sem, r_sem, to):
        return pltpu.make_async_remote_copy(
            src_ref=src, dst_ref=dst, send_sem=s_sem, recv_sem=r_sem, device_id=to, device_id_type=MESH
        )

    def wait_recv(ref, sem):
        remote(ref, ref, sem, sem, sibling).wait_recv()

    def wait_send(ref, sem):
        remote(ref, ref, sem, sem, sibling).wait_send()

    def peer(i):
        a = i // n_x
        off = n_z // 2 + (1 - 2 * (a % 2)) * ((a + 1) // 2)
        zz = (z + off) % n_z
        xx = (x + 1 + i) % n_x
        return zz // n_zl, (zz % n_zl) * n_x + xx

    loads = [
        pltpu.make_async_copy(gate_hbm, stage_g, load_sem.at[0]),
        pltpu.make_async_copy(up_hbm, stage_u, load_sem.at[1]),
        pltpu.make_async_copy(down_hbm, stage_d, load_sem.at[2]),
    ]
    for copy in loads:
        copy.start()

    barrier = pltpu.get_barrier_semaphore()

    def greet(i, carry):
        pg, pf = peer(i)
        pl.semaphore_signal(barrier, inc=1, device_id=(pg, pf, t), device_id_type=MESH)
        return carry

    lax.fori_loop(0, n_peer - 1, greet, 0)

    def greet_down(i, carry):
        to = (t // n_zl, (t % n_zl) * n_x + i // n_tp, i % n_tp)
        mine = jnp.logical_and(z == t, jnp.logical_and(i // n_tp == x, i % n_tp == t))

        @pl.when(jnp.logical_not(mine))
        def _():
            pl.semaphore_signal(barrier, inc=1, device_id=to, device_id_type=MESH)

        return carry

    lax.fori_loop(0, n_x * n_tp, greet_down, 0)
    for dy in range(1, n_y):
        pl.semaphore_signal(barrier, inc=1, device_id=(g, f, ((y + dy) % n_y) * n_c + c), device_id_type=MESH)
    pl.semaphore_signal(barrier, inc=1, device_id=sibling, device_id_type=MESH)

    n_tok = tok_ref.shape[0]
    ids = ids_ref[...]
    sig = jax.nn.sigmoid(logit_ref[...])
    share = sig / jnp.sum(sig, axis=0, keepdims=True)
    experts = lax.broadcasted_iota(jnp.int32, (n_fs, n_tok), 0)
    hit0 = (ids[0:1, :] == experts).astype(F32)
    hit1 = (ids[1:2, :] == experts).astype(F32)
    member = hit0 + hit1
    weight = hit0 * share[0:1, :] + hit1 * share[1:2, :]
    earlier = (
        lax.broadcasted_iota(jnp.int32, (n_tok, n_tok), 0) < lax.broadcasted_iota(jnp.int32, (n_tok, n_tok), 1)
    ).astype(BF16)
    rank = jnp.dot(member.astype(BF16), earlier, preferred_element_type=F32)
    rank = jnp.where(member > 0.5, rank, -1.0)
    slot_no = lax.broadcasted_iota(jnp.int32, (cap, n_tok), 0).astype(F32)
    tok = tok_ref[...]
    for e in range(n_fs):
        pick = (slot_no == rank[e : e + 1, :]).astype(F32)
        slots[e * cap : (e + 1) * cap, :] = jnp.dot(
            pick.astype(BF16), tok, preferred_element_type=F32
        ).astype(BF16)
        scaled = pick * weight[e : e + 1, :]
        hi = scaled.astype(BF16)
        share_hi[e * cap : (e + 1) * cap, :] = hi
        share_lo[e * cap : (e + 1) * cap, :] = (scaled - hi.astype(F32)).astype(BF16)

    gcol = jnp.broadcast_to(gain_ref[...], (rows_g, rows_g)).T
    loads[0].wait()

    def cast_gate(e, carry):
        for h in range(0, stage_g.shape[2], rows_g):
            snd_g[e, :, h : h + rows_g] = (stage_g[e, :, h : h + rows_g] * gcol).astype(BF16)
        return carry

    lax.fori_loop(0, n_fs, cast_gate, 0)
    wg[pl.ds(pl.multiple_of(part * rows_g, rows_g), rows_g), :] = snd_g[f]
    loads[1].wait()

    def cast_up(e, carry):
        for h in range(0, stage_u.shape[2], rows_g):
            snd_u[e, :, h : h + rows_g] = (stage_u[e, :, h : h + rows_g] * gcol).astype(BF16)
        return carry

    lax.fori_loop(0, n_fs, cast_up, 0)
    wu[pl.ds(pl.multiple_of(part * rows_g, rows_g), rows_g), :] = snd_u[f]
    loads[2].wait()

    def cast_down(e, carry):
        for q in range(NQ):
            snd_d[q, e] = stage_d[e, :, q * wq : (q + 1) * wq].astype(BF16)
        return carry

    lax.fori_loop(0, n_fs, cast_down, 0)

    def down_place(q):
        return wd.at[
            pl.ds(pl.multiple_of(x * rows_d, rows_d), rows_d),
            pl.ds(pl.multiple_of(t * wide + q * wq, wq), wq),
        ]

    @pl.when(z == t)
    def _():
        for q in range(NQ):
            wd[
                pl.ds(pl.multiple_of(x * rows_d, rows_d), rows_d),
                pl.ds(pl.multiple_of(t * wide + q * wq, wq), wq),
            ] = snd_d[q, f]

    mine_x = xall.at[t, pl.ds(pl.multiple_of(f * cap, cap), cap), :]
    xall[t, pl.ds(pl.multiple_of(f * cap, cap), cap), :] = slots[pl.ds(pl.multiple_of(f * cap, cap), cap), :]

    pl.semaphore_wait(barrier, (n_peer - 1) + (n_y - 1) + 1 + n_peer - jnp.where(z == t, 1, 0))

    def dispatch(i, carry):
        to = (f + i) % n_fs
        remote(
            slots.at[pl.ds(pl.multiple_of(to * cap, cap), cap), :], mine_x, disp_s, disp_r, (g, to, t)
        ).start()
        return carry

    lax.fori_loop(1, n_fs, dispatch, 0)

    def send_gate(i, carry):
        pg, pf = peer(i)
        remote(
            snd_g.at[pf], wg.at[pl.ds(pl.multiple_of(part * rows_g, rows_g), rows_g), :], w_s.at[0], g_r, (pg, pf, t)
        ).start()
        return carry

    lax.fori_loop(0, n_peer - 1, send_gate, 0)

    wait_recv(xall.at[0, pl.ds(0, (n_fs - 1) * cap), :], disp_r)
    for dy in range(1, n_y):
        remote(xall.at[t], xall.at[t], ag_s, ag_r.at[n_y - dy], (g, f, ((y + dy) % n_y) * n_c + c)).start()
    remote(xall.at[t], xall.at[t], sib_s, sib_r.at[0], sibling).start()

    def send_up(i, carry):
        pg, pf = peer(i)
        remote(
            snd_u.at[pf], wu.at[pl.ds(pl.multiple_of(part * rows_g, rows_g), rows_g), :], w_s.at[1], u_r, (pg, pf, t)
        ).start()
        return carry

    lax.fori_loop(0, n_peer - 1, send_up, 0)
    for q in range(NQ):

        def send_down(i, carry, q=q):
            pg, pf = peer(i)
            remote(snd_d.at[q, pf], down_place(q), w_s.at[2], d_r.at[q], (pg, pf, z)).start()
            return carry

        lax.fori_loop(0, n_peer - 1, send_down, 0)

        @pl.when(z != t)
        def _(q=q):
            remote(snd_d.at[q, f], down_place(q), w_s.at[2], d_r.at[q], (g, f, z)).start()

    for dy in range(1, n_y):
        from_tp = ((y + dy) % n_y) * n_c + c
        wait_recv(xall.at[from_tp], ag_r.at[dy])
        remote(xall.at[from_tp], xall.at[from_tp], sib_s, sib_r.at[dy], sibling).start()
    for dy in range(n_y):
        from_tp = ((y + dy) % n_y) * n_c + (1 - c)
        wait_recv(xall.at[from_tp], sib_r.at[dy])
    wait_send(xall.at[pl.ds(0, n_y - 1)], ag_s)
    wait_send(xall.at[pl.ds(0, n_y)], sib_s)

    row_block = 32

    def normalize(i, carry):
        rows = pl.ds(pl.multiple_of(i * row_block, row_block), row_block)
        squares = jnp.zeros((row_block, wide), F32)
        for k in range(n_tp):
            v = xall[k, rows, :].astype(F32)
            squares = squares + v * v
        scale = lax.rsqrt(jnp.sum(squares, axis=1, keepdims=True) / d_model + EPS)
        for k in range(n_tp):
            xall[k, rows, :] = (xall[k, rows, :].astype(F32) * scale).astype(BF16)
        return carry

    lax.fori_loop(0, n_rows // row_block, normalize, 0)

    all_but_one = (n_peer - 1) * rows_g
    wait_recv(wg.at[pl.ds(0, all_but_one), :], g_r)
    gate_copy = pltpu.make_async_copy(wg, gate_out.at[0], out_sem.at[0])
    gate_copy.start()
    wait_recv(wu.at[pl.ds(0, all_but_one), :], u_r)
    up_copy = pltpu.make_async_copy(wu, up_out.at[0], out_sem.at[1])
    up_copy.start()
    scale_in = d_model ** (-0.5)
    mm_rows = 256

    def hidden_rows(i, carry):
        rows = pl.ds(pl.multiple_of(i * mm_rows, mm_rows), mm_rows)
        gate_sum = jnp.zeros((mm_rows, wg.shape[1]), F32)
        up_sum = jnp.zeros((mm_rows, wu.shape[1]), F32)
        for k in range(n_tp):
            v = xall[k, rows, :]
            gate_sum = gate_sum + jnp.dot(v, wg[k * wide : (k + 1) * wide, :], preferred_element_type=F32)
            up_sum = up_sum + jnp.dot(v, wu[k * wide : (k + 1) * wide, :], preferred_element_type=F32)
        gate_value = gate_sum * scale_in
        hidden[rows, :] = (gate_value * jax.nn.sigmoid(gate_value) * (up_sum * scale_in)).astype(BF16)
        return carry

    lax.fori_loop(0, n_rows // mm_rows, hidden_rows, 0)

    scale_out = (n_tp * wg.shape[1]) ** (-0.5)

    def partial(q, col_tp):
        cols = pl.ds(pl.multiple_of(col_tp * wide + q * wq, wq), wq)
        return jnp.dot(hidden[...], wd[:, cols], preferred_element_type=F32)

    def finish(q):
        for dy in range(1, n_y):
            wait_recv(yrecv.at[q, dy], ys_r.at[q, dy])
        total = ysum[q, y].astype(F32)
        for dy in range(1, n_y):
            total = total + yrecv[q, dy].astype(F32)
        rsend[q] = (total * scale_out).astype(BF16)

        rrecv[q, pl.ds(pl.multiple_of(f * cap, cap), cap), :] = rsend[q, pl.ds(pl.multiple_of(f * cap, cap), cap), :]

        def give(i, carry):
            to = (f + i) % n_fs
            remote(
                rsend.at[q, pl.ds(pl.multiple_of(to * cap, cap), cap), :],
                rrecv.at[q, pl.ds(pl.multiple_of(f * cap, cap), cap), :],
                rt_s, rt_r.at[q], (g, to, t),
            ).start()
            return carry

        lax.fori_loop(1, n_fs, give, 0)

    def combine(q):
        wait_recv(rrecv.at[q, pl.ds(0, (n_fs - 1) * cap), :], rt_r.at[q])
        dn = (((0,), (0,)), ((), ()))
        got = rrecv[q]
        out = lax.dot_general(share_hi[...], got, dn, preferred_element_type=F32)
        out = out + lax.dot_general(share_lo[...], got, dn, preferred_element_type=F32)
        mixed_out[:, q * wq : (q + 1) * wq] = out.astype(BF16)

    for q in range(NQ):

        @pl.when(z == t)
        def _(q=q):
            wait_recv(wg.at[pl.ds(0, all_but_one // NQ), :], d_r.at[q])

        @pl.when(z != t)
        def _(q=q):
            wait_recv(wg.at[pl.ds(0, wg.shape[0] // NQ), :], d_r.at[q])

        def for_sibling(yy, carry, q=q):
            psend[q, yy] = partial(q, yy * n_c + (1 - c)).astype(BF16)
            return carry

        lax.fori_loop(0, n_y, for_sibling, 0)
        remote(psend.at[q], precv.at[q], ps_s, ps_r.at[q], sibling).start()

        def for_own(yy, carry, q=q):
            ysum[q, yy] = partial(q, yy * n_c + c).astype(BF16)
            return carry

        lax.fori_loop(0, n_y, for_own, 0)
        if q > 0:
            finish(q - 1)
        wait_recv(precv.at[q], ps_r.at[q])

        def pair_sum(yy, carry, q=q):
            ysum[q, yy] = (ysum[q, yy].astype(F32) + precv[q, yy].astype(F32)).astype(BF16)
            return carry

        lax.fori_loop(0, n_y, pair_sum, 0)
        for dy in (2, 1, 3):
            yy = (y + dy) % n_y
            remote(ysum.at[q, yy], yrecv.at[q, n_y - dy], ys_s, ys_r.at[q, n_y - dy], (g, f, yy * n_c + c)).start()
        if q > 1:
            combine(q - 2)
    down_copy = pltpu.make_async_copy(wd, down_out.at[0], out_sem.at[2])
    down_copy.start()
    finish(NQ - 1)
    for q in range(max(NQ - 2, 0), NQ):
        combine(q)

    wait_send(slots.at[pl.ds(0, (n_fs - 1) * cap), :], disp_s)
    wait_send(wg.at[pl.ds(0, all_but_one), :], w_s.at[0])
    wait_send(wu.at[pl.ds(0, all_but_one), :], w_s.at[1])

    @pl.when(z == t)
    def _():
        wait_send(wg.at[pl.ds(0, all_but_one), :], w_s.at[2])

    @pl.when(z != t)
    def _():
        wait_send(wg, w_s.at[2])

    wait_send(psend, ps_s)
    wait_send(yrecv.at[:, pl.ds(0, n_y - 1)], ys_s)
    wait_send(rrecv.at[:, pl.ds(0, (n_fs - 1) * cap), :], rt_s)
    gate_copy.wait()
    up_copy.wait()
    down_copy.wait()


def body(tokens, route_ids, route_logits, gain, gate_master, up_master, down_master, *, sizes):
    n_gr, n_zl, n_x, n_y, n_c = sizes
    experts, rows_g, ff = gate_master.shape
    rows_d, wide = down_master.shape[1:]
    n_tok, top = route_ids.shape
    cap = 2 * n_tok * top // experts
    n_fs, n_tp = n_zl * n_x, n_y * n_c
    n_rows = n_fs * cap
    d_model, hid = wide * n_tp, ff
    wq = wide // NQ
    vmem = lambda *shape, dtype=BF16: pltpu.VMEM(shape, dtype)
    dma = pltpu.SemaphoreType.DMA
    any_spec = pl.BlockSpec(memory_space=pl.ANY)
    vmem_spec = pl.BlockSpec(memory_space=pltpu.VMEM)
    return pl.pallas_call(
        functools.partial(kernel, (n_gr, n_zl, n_x, n_y, n_c, cap)),
        out_shape=(
            jax.ShapeDtypeStruct((1, d_model, ff), BF16),
            jax.ShapeDtypeStruct((1, d_model, ff), BF16),
            jax.ShapeDtypeStruct((1, hid, d_model), BF16),
            jax.ShapeDtypeStruct((n_tok, wide), BF16),
        ),
        in_specs=[vmem_spec] * 4 + [any_spec] * 3,
        out_specs=(any_spec, any_spec, any_spec, vmem_spec),
        scratch_shapes=[
            vmem(experts, rows_g, ff, dtype=F32),
            vmem(experts, rows_g, ff, dtype=F32),
            vmem(experts, rows_d, wide, dtype=F32),
            vmem(experts, rows_g, ff),
            vmem(experts, rows_g, ff),
            vmem(NQ, experts, rows_d, wq),
            vmem(d_model, ff),
            vmem(d_model, ff),
            vmem(hid, d_model),
            vmem(n_rows, wide),
            vmem(n_rows, n_tok),
            vmem(n_rows, n_tok),
            vmem(n_tp, n_rows, wide),
            vmem(n_rows, hid),
            vmem(NQ, n_y, n_rows, wq),
            vmem(NQ, n_y, n_rows, wq),
            vmem(NQ, n_y, n_rows, wq),
            vmem(NQ, n_y, n_rows, wq),
            vmem(NQ, n_rows, wq),
            vmem(NQ, n_rows, wq),
            dma((3,)), dma, dma, dma((3,)), dma, dma, dma((NQ,)),
            dma, dma((n_y,)), dma, dma((n_y,)), dma, dma((NQ,)), dma, dma((NQ, n_y)), dma, dma((NQ,)), dma((3,)),
        ],
        compiler_params=pltpu.CompilerParams(
            collective_id=0, has_side_effects=True, vmem_limit_bytes=60 * 1024 * 1024
        ),
    )(tokens, route_ids.T, route_logits.T, gain[None, :], gate_master, up_master, down_master)


def solution(mesh):
    n_zl, n_x, n_c = 4, 4, 2
    sizes = (mesh.shape["gr"], n_zl, n_x, mesh.shape["tp"] // n_c, n_c)
    in_specs = (
        P(("gr", "fs"), "tp"),
        P(("gr", "fs"), None),
        P(("gr", "fs"), None),
        P(("gr", "fs")),
        P(None, ("gr", "fs"), "tp"),
        P(None, ("gr", "fs"), "tp"),
        P(None, ("gr", "fs"), "tp"),
    )
    out_specs = (
        P("fs", None, "tp"),
        P("fs", None, "tp"),
        P("fs", "tp", None),
        P(("gr", "fs"), "tp"),
    )
    return jax.shard_map(
        functools.partial(body, sizes=sizes), mesh=mesh, in_specs=in_specs, out_specs=out_specs, check_vma=False
    )
```

```python
import functools

import jax
import jax.numpy as jnp
from jax import lax
from jax.experimental import pallas as pl
from jax.experimental.pallas import tpu as pltpu
from jax.sharding import PartitionSpec as P

EPS = 1e-06
MESH = pl.DeviceIdType.MESH
F32 = jnp.float32
BF16 = jnp.bfloat16
NQ = 4
NR = 4


def kernel(
    dims,
    tok_ref, ids_ref, logit_ref, gain_ref, gate_hbm, up_hbm, down_hbm,
    wg_out, wu_out, wd_out, mixed_out,
    stage_g, stage_u, stage_d, snd_g, snd_u, snd_d,
    slots, share_hi, share_lo, xall, hidden,
    psend, precv, ysum, yrecv, rsend, rrecv,
    load_sem, disp_s, disp_r, w_s, g_r, u_r, d_r,
    ag_s, ag_r, sib_s, sib_r, ps_s, ps_r, ys_s, ys_r, rt_s, rt_r,
):
    n_gr, n_zl, n_x, n_y, n_c, cap = dims
    wg, wu, wd = wg_out.at[0], wu_out.at[0], wd_out.at[0]
    n_fs = n_zl * n_x
    n_z = n_gr * n_zl
    n_tp = n_y * n_c
    g = lax.axis_index("gr")
    f = lax.axis_index("fs")
    t = lax.axis_index("tp")
    z = g * n_zl + f // n_x
    x = f % n_x
    y = t // n_c
    c = t % n_c
    part = g * n_fs + f
    rows_g = stage_g.shape[1]
    rows_d = stage_d.shape[1]
    wide = tok_ref.shape[1]
    wq = wide // NQ
    n_rows = n_fs * cap
    n_peer = n_z * n_x
    d_model = n_tp * wide
    sibling = (g, f, y * n_c + (1 - c))

    def remote(src, dst, s_sem, r_sem, to):
        return pltpu.make_async_remote_copy(
            src_ref=src, dst_ref=dst, send_sem=s_sem, recv_sem=r_sem, device_id=to, device_id_type=MESH
        )

    def wait_recv(ref, sem):
        remote(ref, ref, sem, sem, sibling).wait_recv()

    def wait_send(ref, sem):
        remote(ref, ref, sem, sem, sibling).wait_send()

    def peer(i, turn=0):
        a = i % n_z
        off = n_z // 2 + (1 - 2 * (a % 2)) * ((a + 1) // 2)
        zz = (z + off) % n_z
        xx = (x + 1 + i // n_z + turn) % n_x
        return zz // n_zl, (zz % n_zl) * n_x + xx

    loads = [
        pltpu.make_async_copy(gate_hbm, stage_g, load_sem.at[0]),
        pltpu.make_async_copy(up_hbm, stage_u, load_sem.at[1]),
        pltpu.make_async_copy(down_hbm, stage_d, load_sem.at[2]),
    ]
    for copy in loads:
        copy.start()

    barrier = pltpu.get_barrier_semaphore()

    def greet(i, carry):
        pg, pf = peer(i)
        pl.semaphore_signal(barrier, inc=1, device_id=(pg, pf, t), device_id_type=MESH)
        return carry

    lax.fori_loop(0, n_peer - 1, greet, 0)

    def greet_down(i, carry):
        to = (t // n_zl, (t % n_zl) * n_x + i // n_tp, i % n_tp)
        mine = jnp.logical_and(z == t, jnp.logical_and(i // n_tp == x, i % n_tp == t))

        @pl.when(jnp.logical_not(mine))
        def _():
            pl.semaphore_signal(barrier, inc=1, device_id=to, device_id_type=MESH)

        return carry

    lax.fori_loop(0, n_x * n_tp, greet_down, 0)
    for dy in range(1, n_y):
        pl.semaphore_signal(barrier, inc=1, device_id=(g, f, ((y + dy) % n_y) * n_c + c), device_id_type=MESH)
    pl.semaphore_signal(barrier, inc=1, device_id=sibling, device_id_type=MESH)

    n_tok = tok_ref.shape[0]
    ids = ids_ref[...]
    sig = jax.nn.sigmoid(logit_ref[...])
    share = sig / jnp.sum(sig, axis=0, keepdims=True)
    experts = lax.broadcasted_iota(jnp.int32, (n_fs, n_tok), 0)
    hit0 = (ids[0:1, :] == experts).astype(F32)
    hit1 = (ids[1:2, :] == experts).astype(F32)
    member = hit0 + hit1
    weight = hit0 * share[0:1, :] + hit1 * share[1:2, :]
    earlier = (
        lax.broadcasted_iota(jnp.int32, (n_tok, n_tok), 0) < lax.broadcasted_iota(jnp.int32, (n_tok, n_tok), 1)
    ).astype(BF16)
    rank = jnp.dot(member.astype(BF16), earlier, preferred_element_type=F32)
    rank = jnp.where(member > 0.5, rank, -1.0)
    slot_no = lax.broadcasted_iota(jnp.int32, (cap, n_tok), 0).astype(F32)
    tok = tok_ref[...]
    for e in range(n_fs):
        pick = (slot_no == rank[e : e + 1, :]).astype(F32)
        slots[e * cap : (e + 1) * cap, :] = jnp.dot(
            pick.astype(BF16), tok, preferred_element_type=F32
        ).astype(BF16)
        scaled = pick * weight[e : e + 1, :]
        hi = scaled.astype(BF16)
        share_hi[e * cap : (e + 1) * cap, :] = hi
        share_lo[e * cap : (e + 1) * cap, :] = (scaled - hi.astype(F32)).astype(BF16)

    gcol = jnp.broadcast_to(gain_ref[...], (rows_g, rows_g)).T
    loads[0].wait()

    def cast_gate(e, carry):
        for h in range(0, stage_g.shape[2], rows_g):
            snd_g[e, :, h : h + rows_g] = (stage_g[e, :, h : h + rows_g] * gcol).astype(BF16)
        return carry

    lax.fori_loop(0, n_fs, cast_gate, 0)
    wg[pl.ds(pl.multiple_of(part * rows_g, rows_g), rows_g), :] = snd_g[f]
    loads[1].wait()

    def cast_up(e, carry):
        for h in range(0, stage_u.shape[2], rows_g):
            snd_u[e, :, h : h + rows_g] = (stage_u[e, :, h : h + rows_g] * gcol).astype(BF16)
        return carry

    lax.fori_loop(0, n_fs, cast_up, 0)
    wu[pl.ds(pl.multiple_of(part * rows_g, rows_g), rows_g), :] = snd_u[f]
    loads[2].wait()

    def cast_down(e, carry):
        for q in range(NQ):
            snd_d[q, e] = stage_d[e, :, q * wq : (q + 1) * wq].astype(BF16)
        return carry

    lax.fori_loop(0, n_fs, cast_down, 0)

    def down_place(q):
        return wd.at[
            pl.ds(pl.multiple_of(x * rows_d, rows_d), rows_d),
            pl.ds(pl.multiple_of(t * wide + q * wq, wq), wq),
        ]

    @pl.when(z == t)
    def _():
        for q in range(NQ):
            wd[
                pl.ds(pl.multiple_of(x * rows_d, rows_d), rows_d),
                pl.ds(pl.multiple_of(t * wide + q * wq, wq), wq),
            ] = snd_d[q, f]

    mine_x = xall.at[t, pl.ds(pl.multiple_of(f * cap, cap), cap), :]
    xall[t, pl.ds(pl.multiple_of(f * cap, cap), cap), :] = slots[pl.ds(pl.multiple_of(f * cap, cap), cap), :]

    pl.semaphore_wait(barrier, (n_peer - 1) + (n_y - 1) + 1 + n_peer - jnp.where(z == t, 1, 0))

    def dispatch(i, carry):
        to = (f + i) % n_fs
        remote(
            slots.at[pl.ds(pl.multiple_of(to * cap, cap), cap), :], mine_x, disp_s, disp_r, (g, to, t)
        ).start()
        return carry

    lax.fori_loop(1, n_fs, dispatch, 0)

    def send_gate(i, carry):
        pg, pf = peer(i)
        remote(
            snd_g.at[pf], wg.at[pl.ds(pl.multiple_of(part * rows_g, rows_g), rows_g), :], w_s.at[0], g_r, (pg, pf, t)
        ).start()
        return carry

    lax.fori_loop(0, n_peer - 1, send_gate, 0)

    wait_recv(xall.at[0, pl.ds(0, (n_fs - 1) * cap), :], disp_r)
    for dy in range(1, n_y):
        remote(xall.at[t], xall.at[t], ag_s, ag_r.at[n_y - dy], (g, f, ((y + dy) % n_y) * n_c + c)).start()
    remote(xall.at[t], xall.at[t], sib_s, sib_r.at[0], sibling).start()

    def send_up(i, carry):
        pg, pf = peer(i)
        remote(
            snd_u.at[pf], wu.at[pl.ds(pl.multiple_of(part * rows_g, rows_g), rows_g), :], w_s.at[1], u_r, (pg, pf, t)
        ).start()
        return carry

    lax.fori_loop(0, n_peer - 1, send_up, 0)
    for dy in range(1, n_y):
        from_tp = ((y + dy) % n_y) * n_c + c
        wait_recv(xall.at[from_tp], ag_r.at[dy])
        remote(xall.at[from_tp], xall.at[from_tp], sib_s, sib_r.at[dy], sibling).start()
    for dy in range(n_y):
        from_tp = ((y + dy) % n_y) * n_c + (1 - c)
        wait_recv(xall.at[from_tp], sib_r.at[dy])
    wait_send(xall.at[pl.ds(0, n_y - 1)], ag_s)
    wait_send(xall.at[pl.ds(0, n_y)], sib_s)

    row_block = 32

    def normalize(i, carry):
        rows = pl.ds(pl.multiple_of(i * row_block, row_block), row_block)
        squares = jnp.zeros((row_block, wide), F32)
        for k in range(n_tp):
            v = xall[k, rows, :].astype(F32)
            squares = squares + v * v
        scale = lax.rsqrt(jnp.sum(squares, axis=1, keepdims=True) / d_model + EPS)
        for k in range(n_tp):
            xall[k, rows, :] = (xall[k, rows, :].astype(F32) * scale).astype(BF16)
        return carry

    lax.fori_loop(0, n_rows // row_block, normalize, 0)

    def start_down(q):
        def send_down(i, carry):
            pg, pf = peer(i, y)
            here = jnp.logical_and(jnp.logical_and(pg == g, pf == f), t == z)

            @pl.when(jnp.logical_not(here))
            def _():
                remote(snd_d.at[q, pf], down_place(q), w_s.at[2], d_r.at[q], (pg, pf, z)).start()

            return carry

        lax.fori_loop(0, n_peer, send_down, 0)

    for q in range(2):
        start_down(q)

    all_but_one = (n_peer - 1) * rows_g
    wait_recv(wg.at[pl.ds(0, all_but_one), :], g_r)
    wait_recv(wu.at[pl.ds(0, all_but_one), :], u_r)
    scale_in = d_model ** (-0.5)
    mm_rows = 256

    def hidden_rows(i, carry):
        rows = pl.ds(pl.multiple_of(i * mm_rows, mm_rows), mm_rows)
        gate_sum = jnp.zeros((mm_rows, wg.shape[1]), F32)
        up_sum = jnp.zeros((mm_rows, wu.shape[1]), F32)
        for k in range(n_tp):
            v = xall[k, rows, :]
            gate_sum = gate_sum + jnp.dot(v, wg[k * wide : (k + 1) * wide, :], preferred_element_type=F32)
            up_sum = up_sum + jnp.dot(v, wu[k * wide : (k + 1) * wide, :], preferred_element_type=F32)
        gate_value = gate_sum * scale_in
        hidden[rows, :] = (gate_value * jax.nn.sigmoid(gate_value) * (up_sum * scale_in)).astype(BF16)
        return carry

    lax.fori_loop(0, n_rows // mm_rows, hidden_rows, 0)

    scale_out = (n_tp * wg.shape[1]) ** (-0.5)

    piece = n_rows // NR
    per_piece = n_fs // NR

    def partial(q, r, col_tp):
        rows = pl.ds(pl.multiple_of(r * piece, piece), piece)
        cols = pl.ds(pl.multiple_of(col_tp * wide + q * wq, wq), wq)
        return jnp.dot(hidden[rows, :], wd[:, cols], preferred_element_type=F32)

    def finish(q):
        def one(r, carry):
            wait_recv(yrecv.at[q, r, pl.ds(0, n_y - 1)], ys_r.at[q, r])
            total = ysum[q, r, y].astype(F32)
            for dy in range(1, n_y):
                total = total + yrecv[q, r, dy].astype(F32)
            rsend[q, pl.ds(pl.multiple_of(r * piece, piece), piece), :] = (total * scale_out).astype(BF16)

            def give(i, carry):
                to = r * per_piece + i
                block = pl.ds(pl.multiple_of(to * cap, cap), cap)
                mine = pl.ds(pl.multiple_of(f * cap, cap), cap)

                @pl.when(to == f)
                def _():
                    rrecv[q, mine, :] = rsend[q, mine, :]

                @pl.when(to != f)
                def _():
                    remote(rsend.at[q, block, :], rrecv.at[q, mine, :], rt_s, rt_r.at[q], (g, to, t)).start()

                return carry

            lax.fori_loop(0, per_piece, give, 0)
            return carry

        lax.fori_loop(0, NR, one, 0)

    def combine(q):
        wait_recv(rrecv.at[q, pl.ds(0, (n_fs - 1) * cap), :], rt_r.at[q])
        dn = (((0,), (0,)), ((), ()))
        got = rrecv[q]
        out = lax.dot_general(share_hi[...], got, dn, preferred_element_type=F32)
        out = out + lax.dot_general(share_lo[...], got, dn, preferred_element_type=F32)
        mixed_out[:, q * wq : (q + 1) * wq] = out.astype(BF16)

    for q in range(NQ):

        @pl.when(z == t)
        def _(q=q):
            wait_recv(wg.at[pl.ds(0, all_but_one // NQ), :], d_r.at[q])

        @pl.when(z != t)
        def _(q=q):
            wait_recv(wg.at[pl.ds(0, wg.shape[0] // NQ), :], d_r.at[q])

        def for_sibling(r, carry, q=q):
            for yy in range(n_y):
                psend[q, r, yy] = partial(q, r, yy * n_c + (1 - c)).astype(BF16)
            remote(psend.at[q, r], precv.at[q, r], ps_s, ps_r.at[q, r], sibling).start()
            return carry

        if q + 2 < NQ:
            start_down(q + 2)
        lax.fori_loop(0, NR, for_sibling, 0)

        def for_own(r, carry, q=q):
            for yy in range(n_y):
                ysum[q, r, yy] = partial(q, r, yy * n_c + c).astype(BF16)
            return carry

        lax.fori_loop(0, NR, for_own, 0)
        if q > 0:
            finish(q - 1)

        def exchange(r, carry, q=q):
            wait_recv(precv.at[q, r], ps_r.at[q, r])
            for yy in range(n_y):
                ysum[q, r, yy] = (ysum[q, r, yy].astype(F32) + precv[q, r, yy].astype(F32)).astype(BF16)
            for dy in (2, 1, 3):
                yy = (y + dy) % n_y
                remote(
                    ysum.at[q, r, yy], yrecv.at[q, r, n_y - dy], ys_s, ys_r.at[q, r], (g, f, yy * n_c + c)
                ).start()
            return carry

        lax.fori_loop(0, NR, exchange, 0)
        if q > 1:
            combine(q - 2)
    finish(NQ - 1)
    for q in range(max(NQ - 2, 0), NQ):
        combine(q)

    wait_send(slots.at[pl.ds(0, (n_fs - 1) * cap), :], disp_s)
    wait_send(wg.at[pl.ds(0, all_but_one), :], w_s.at[0])
    wait_send(wu.at[pl.ds(0, all_but_one), :], w_s.at[1])

    @pl.when(z == t)
    def _():
        wait_send(wg.at[pl.ds(0, all_but_one), :], w_s.at[2])

    @pl.when(z != t)
    def _():
        wait_send(wg, w_s.at[2])

    wait_send(psend, ps_s)
    wait_send(yrecv.at[:, :, pl.ds(0, n_y - 1)], ys_s)
    wait_send(rrecv.at[:, pl.ds(0, (n_fs - 1) * cap), :], rt_s)


def write_out(*refs):
    n = len(refs) // 2
    srcs, dsts, sem = refs[:n], refs[n : 2 * n], refs[2 * n]
    copies = [pltpu.make_async_copy(src, dst, sem.at[i]) for i, (src, dst) in enumerate(zip(srcs, dsts))]
    for copy in copies:
        copy.start()
    for copy in copies:
        copy.wait()


def body(tokens, route_ids, route_logits, gain, gate_master, up_master, down_master, *, sizes):
    n_gr, n_zl, n_x, n_y, n_c = sizes
    experts, rows_g, ff = gate_master.shape
    rows_d, wide = down_master.shape[1:]
    n_tok, top = route_ids.shape
    cap = 2 * n_tok * top // experts
    n_fs, n_tp = n_zl * n_x, n_y * n_c
    n_rows = n_fs * cap
    d_model, hid = wide * n_tp, ff
    wq = wide // NQ
    vmem = lambda *shape, dtype=BF16: pltpu.VMEM(shape, dtype)
    dma = pltpu.SemaphoreType.DMA
    any_spec = pl.BlockSpec(memory_space=pl.ANY)
    vmem_spec = pl.BlockSpec(memory_space=pltpu.VMEM)
    results = pl.pallas_call(
        functools.partial(kernel, (n_gr, n_zl, n_x, n_y, n_c, cap)),
        out_shape=(
            pltpu.VMEM((1, d_model, ff), BF16),
            pltpu.VMEM((1, d_model, ff), BF16),
            pltpu.VMEM((1, hid, d_model), BF16),
            pltpu.VMEM((n_tok, wide), BF16),
        ),
        in_specs=[vmem_spec] * 4 + [any_spec] * 3,
        out_specs=(vmem_spec,) * 4,
        scratch_shapes=[
            vmem(experts, rows_g, ff, dtype=F32),
            vmem(experts, rows_g, ff, dtype=F32),
            vmem(experts, rows_d, wide, dtype=F32),
            vmem(experts, rows_g, ff),
            vmem(experts, rows_g, ff),
            vmem(NQ, experts, rows_d, wq),
            vmem(n_rows, wide),
            vmem(n_rows, n_tok),
            vmem(n_rows, n_tok),
            vmem(n_tp, n_rows, wide),
            vmem(n_rows, hid),
            vmem(NQ, NR, n_y, n_rows // NR, wq),
            vmem(NQ, NR, n_y, n_rows // NR, wq),
            vmem(NQ, NR, n_y, n_rows // NR, wq),
            vmem(NQ, NR, n_y, n_rows // NR, wq),
            vmem(NQ, n_rows, wq),
            vmem(NQ, n_rows, wq),
            dma((3,)), dma, dma, dma((3,)), dma, dma, dma((NQ,)),
            dma, dma((n_y,)), dma, dma((n_y,)), dma, dma((NQ, NR)), dma, dma((NQ, NR)), dma, dma((NQ,)),
        ],
        compiler_params=pltpu.CompilerParams(
            collective_id=0, has_side_effects=True, vmem_limit_bytes=50 * 1024 * 1024
        ),
    )(tokens, route_ids.T, route_logits.T, gain[None, :], gate_master, up_master, down_master)
    return pl.pallas_call(
        write_out,
        out_shape=tuple(jax.ShapeDtypeStruct(r.shape, r.dtype) for r in results),
        in_specs=[vmem_spec] * 4,
        out_specs=(any_spec,) * 4,
        scratch_shapes=[dma((4,))],
        compiler_params=pltpu.CompilerParams(vmem_limit_bytes=1024 * 1024),
    )(*(pltpu.with_memory_space_constraint(r, pltpu.VMEM) for r in results))


def solution(mesh):
    n_zl, n_x, n_c = 4, 4, 2
    sizes = (mesh.shape["gr"], n_zl, n_x, mesh.shape["tp"] // n_c, n_c)
    in_specs = (
        P(("gr", "fs"), "tp"),
        P(("gr", "fs"), None),
        P(("gr", "fs"), None),
        P(("gr", "fs")),
        P(None, ("gr", "fs"), "tp"),
        P(None, ("gr", "fs"), "tp"),
        P(None, ("gr", "fs"), "tp"),
    )
    out_specs = (
        P("fs", None, "tp"),
        P("fs", None, "tp"),
        P("fs", "tp", None),
        P(("gr", "fs"), "tp"),
    )
    return jax.shard_map(
        functools.partial(body, sizes=sizes), mesh=mesh, in_specs=in_specs, out_specs=out_specs, check_vma=False
    )
```

```python
import functools

import jax
import jax.numpy as jnp
from jax import lax
from jax.experimental import pallas as pl
from jax.experimental.pallas import tpu as pltpu
from jax.sharding import PartitionSpec as P

EPS = 1e-06
MESH = pl.DeviceIdType.MESH
F32 = jnp.float32
BF16 = jnp.bfloat16
NQ = 4
NR = 4


def kernel(
    dims,
    tok_hbm, ids_hbm, logit_hbm, gain_hbm, gate_hbm, up_hbm, down_hbm,
    wg_out, wu_out, wd_out, mixed_out,
    stage_g, stage_u, stage_d, snd_g, snd_u, snd_d,
    slots, share_hi, share_lo, xall, gate_act, hidden,
    tok_ref, ids_ref, logit_ref, gain_ref,
    psend, precv, ysum, passing, yrecv, rsend, rrecv,
    load_sem, disp_s, disp_r, w_s, g_r, u_r, d_r,
    ag_s, ag_r, sib_s, sib_r, ps_s, ps_r, ys_s, ps_y, ys_r, rt_s, rt_r,
):
    n_gr, n_zl, n_x, n_y, n_c, cap = dims
    wg, wu, wd = wg_out.at[0], wu_out.at[0], wd_out.at[0]
    n_fs = n_zl * n_x
    n_z = n_gr * n_zl
    n_tp = n_y * n_c
    g = lax.axis_index("gr")
    f = lax.axis_index("fs")
    t = lax.axis_index("tp")
    z = g * n_zl + f // n_x
    x = f % n_x
    y = t // n_c
    c = t % n_c
    part = g * n_fs + f
    rows_g = stage_g.shape[1]
    rows_d = stage_d.shape[1]
    wide = tok_ref.shape[1]
    wq = wide // NQ
    n_rows = n_fs * cap
    n_peer = n_z * n_x
    d_model = n_tp * wide
    sibling = (g, f, y * n_c + (1 - c))

    def remote(src, dst, s_sem, r_sem, to):
        return pltpu.make_async_remote_copy(
            src_ref=src, dst_ref=dst, send_sem=s_sem, recv_sem=r_sem, device_id=to, device_id_type=MESH
        )

    def wait_recv(ref, sem):
        remote(ref, ref, sem, sem, sibling).wait_recv()

    def wait_send(ref, sem):
        remote(ref, ref, sem, sem, sibling).wait_send()

    def peer(i, turn=0):
        a = i % n_z
        off = n_z // 2 + (1 - 2 * (a % 2)) * ((a + 1) // 2)
        zz = (z + off) % n_z
        xx = (x + 1 + i // n_z + turn) % n_x
        return zz // n_zl, (zz % n_zl) * n_x + xx

    loads = [
        pltpu.make_async_copy(gate_hbm, stage_g, load_sem.at[0]),
        pltpu.make_async_copy(up_hbm, stage_u, load_sem.at[1]),
        pltpu.make_async_copy(down_hbm, stage_d, load_sem.at[2]),
    ]
    small = [
        pltpu.make_async_copy(src, dst, load_sem.at[3 + i])
        for i, (src, dst) in enumerate(
            ((tok_hbm, tok_ref), (ids_hbm, ids_ref), (logit_hbm, logit_ref), (gain_hbm, gain_ref))
        )
    ]
    for copy in small + loads:
        copy.start()

    barrier = pltpu.get_barrier_semaphore()

    def greet(i, carry):
        pg, pf = peer(i)
        pl.semaphore_signal(barrier, inc=1, device_id=(pg, pf, t), device_id_type=MESH)
        return carry

    lax.fori_loop(0, n_peer - 1, greet, 0)

    def greet_down(i, carry):
        to = (t // n_zl, (t % n_zl) * n_x + i // n_tp, i % n_tp)
        mine = jnp.logical_and(z == t, jnp.logical_and(i // n_tp == x, i % n_tp == t))

        @pl.when(jnp.logical_not(mine))
        def _():
            pl.semaphore_signal(barrier, inc=1, device_id=to, device_id_type=MESH)

        return carry

    lax.fori_loop(0, n_x * n_tp, greet_down, 0)
    for dy in range(1, n_y):
        pl.semaphore_signal(barrier, inc=1, device_id=(g, f, ((y + dy) % n_y) * n_c + c), device_id_type=MESH)
    pl.semaphore_signal(barrier, inc=1, device_id=sibling, device_id_type=MESH)

    for copy in small:
        copy.wait()
    n_tok = tok_ref.shape[0]
    ids = ids_ref[...]
    sig = jax.nn.sigmoid(logit_ref[...])
    share = sig / jnp.sum(sig, axis=0, keepdims=True)
    experts = lax.broadcasted_iota(jnp.int32, (n_fs, n_tok), 0)
    hit0 = (ids[0:1, :] == experts).astype(F32)
    hit1 = (ids[1:2, :] == experts).astype(F32)
    member = hit0 + hit1
    weight = hit0 * share[0:1, :] + hit1 * share[1:2, :]
    earlier = (
        lax.broadcasted_iota(jnp.int32, (n_tok, n_tok), 0) < lax.broadcasted_iota(jnp.int32, (n_tok, n_tok), 1)
    ).astype(BF16)
    rank = jnp.dot(member.astype(BF16), earlier, preferred_element_type=F32)
    rank = jnp.where(member > 0.5, rank, -1.0)
    slot_no = lax.broadcasted_iota(jnp.int32, (cap, n_tok), 0).astype(F32)
    tok = tok_ref[...]
    for e in range(n_fs):
        pick = (slot_no == rank[e : e + 1, :]).astype(F32)
        slots[e * cap : (e + 1) * cap, :] = jnp.dot(
            pick.astype(BF16), tok, preferred_element_type=F32
        ).astype(BF16)
        scaled = pick * weight[e : e + 1, :]
        hi = scaled.astype(BF16)
        share_hi[e * cap : (e + 1) * cap, :] = hi
        share_lo[e * cap : (e + 1) * cap, :] = (scaled - hi.astype(F32)).astype(BF16)

    gcol = jnp.broadcast_to(gain_ref[...], (rows_g, rows_g)).T
    loads[0].wait()

    def cast_gate(e, carry):
        for h in range(0, stage_g.shape[2], rows_g):
            snd_g[e, :, h : h + rows_g] = (stage_g[e, :, h : h + rows_g] * gcol).astype(BF16)
        return carry

    lax.fori_loop(0, n_fs, cast_gate, 0)
    wg[pl.ds(pl.multiple_of(part * rows_g, rows_g), rows_g), :] = snd_g[f]
    loads[1].wait()

    def cast_up(e, carry):
        for h in range(0, stage_u.shape[2], rows_g):
            snd_u[e, :, h : h + rows_g] = (stage_u[e, :, h : h + rows_g] * gcol).astype(BF16)
        return carry

    lax.fori_loop(0, n_fs, cast_up, 0)
    wu[pl.ds(pl.multiple_of(part * rows_g, rows_g), rows_g), :] = snd_u[f]
    loads[2].wait()

    def cast_down(e, carry):
        for q in range(NQ):
            snd_d[q, e] = stage_d[e, :, q * wq : (q + 1) * wq].astype(BF16)
        return carry

    lax.fori_loop(0, n_fs, cast_down, 0)

    def down_place(q):
        return wd.at[
            pl.ds(pl.multiple_of(x * rows_d, rows_d), rows_d),
            pl.ds(pl.multiple_of(t * wide + q * wq, wq), wq),
        ]

    @pl.when(z == t)
    def _():
        for q in range(NQ):
            wd[
                pl.ds(pl.multiple_of(x * rows_d, rows_d), rows_d),
                pl.ds(pl.multiple_of(t * wide + q * wq, wq), wq),
            ] = snd_d[q, f]

    mine_x = xall.at[t, pl.ds(pl.multiple_of(f * cap, cap), cap), :]
    xall[t, pl.ds(pl.multiple_of(f * cap, cap), cap), :] = slots[pl.ds(pl.multiple_of(f * cap, cap), cap), :]

    pl.semaphore_wait(barrier, (n_peer - 1) + (n_y - 1) + 1 + n_peer - jnp.where(z == t, 1, 0))

    def dispatch(i, carry):
        a = i % n_zl
        off = n_zl // 2 + (2 * (a % 2) - 1) * ((a + 1) // 2)
        to = (f // n_x + off) % n_zl * n_x + (x + 1 + i // n_zl) % n_x
        remote(
            slots.at[pl.ds(pl.multiple_of(to * cap, cap), cap), :], mine_x, disp_s, disp_r, (g, to, t)
        ).start()
        return carry

    lax.fori_loop(0, n_fs - 1, dispatch, 0)

    def send_gate(i, carry):
        pg, pf = peer(i)
        remote(
            snd_g.at[pf], wg.at[pl.ds(pl.multiple_of(part * rows_g, rows_g), rows_g), :], w_s.at[0], g_r, (pg, pf, t)
        ).start()
        return carry

    lax.fori_loop(0, n_peer - 1, send_gate, 0)

    wait_recv(xall.at[0, pl.ds(0, (n_fs - 1) * cap), :], disp_r)
    for dy in range(1, n_y):
        remote(xall.at[t], xall.at[t], ag_s, ag_r.at[n_y - dy], (g, f, ((y + dy) % n_y) * n_c + c)).start()
    remote(xall.at[t], xall.at[t], sib_s, sib_r.at[0], sibling).start()

    def send_up(i, carry):
        pg, pf = peer(i)
        remote(
            snd_u.at[pf], wu.at[pl.ds(pl.multiple_of(part * rows_g, rows_g), rows_g), :], w_s.at[1], u_r, (pg, pf, t)
        ).start()
        return carry

    lax.fori_loop(0, n_peer - 1, send_up, 0)
    for dy in range(1, n_y):
        from_tp = ((y + dy) % n_y) * n_c + c
        wait_recv(xall.at[from_tp], ag_r.at[dy])
        remote(xall.at[from_tp], xall.at[from_tp], sib_s, sib_r.at[dy], sibling).start()
    for dy in range(n_y):
        from_tp = ((y + dy) % n_y) * n_c + (1 - c)
        wait_recv(xall.at[from_tp], sib_r.at[dy])
    wait_send(xall.at[pl.ds(0, n_y - 1)], ag_s)
    wait_send(xall.at[pl.ds(0, n_y)], sib_s)

    row_block = 32

    def normalize(i, carry):
        rows = pl.ds(pl.multiple_of(i * row_block, row_block), row_block)
        squares = jnp.zeros((row_block, wide), F32)
        for k in range(n_tp):
            v = xall[k, rows, :].astype(F32)
            squares = squares + v * v
        scale = lax.rsqrt(jnp.sum(squares, axis=1, keepdims=True) / d_model + EPS)
        for k in range(n_tp):
            xall[k, rows, :] = (xall[k, rows, :].astype(F32) * scale).astype(BF16)
        return carry

    lax.fori_loop(0, n_rows // row_block, normalize, 0)

    def start_down(q):
        def send_down(i, carry):
            pg, pf = peer(i, y)
            here = jnp.logical_and(jnp.logical_and(pg == g, pf == f), t == z)

            @pl.when(jnp.logical_not(here))
            def _():
                remote(snd_d.at[q, pf], down_place(q), w_s.at[2], d_r.at[q], (pg, pf, z)).start()

            return carry

        lax.fori_loop(0, n_peer, send_down, 0)

    for q in range(2):
        start_down(q)

    all_but_one = (n_peer - 1) * rows_g
    wait_recv(wg.at[pl.ds(0, all_but_one), :], g_r)
    scale_in = d_model ** (-0.5)
    mm_rows = 256

    def product(w, rows):
        total = jnp.zeros((mm_rows, w.shape[1]), F32)
        for k in range(n_tp):
            total = total + jnp.dot(xall[k, rows, :], w[k * wide : (k + 1) * wide, :], preferred_element_type=F32)
        return total * scale_in

    def gate_rows(i, carry):
        rows = pl.ds(pl.multiple_of(i * mm_rows, mm_rows), mm_rows)
        gate_value = product(wg, rows)
        gate_act[rows, :] = gate_value * jax.nn.sigmoid(gate_value)
        return carry

    lax.fori_loop(0, n_rows // mm_rows, gate_rows, 0)
    wait_recv(wu.at[pl.ds(0, all_but_one), :], u_r)

    def hidden_rows(i, carry):
        rows = pl.ds(pl.multiple_of(i * mm_rows, mm_rows), mm_rows)
        hidden[rows, :] = (gate_act[rows, :] * product(wu, rows)).astype(BF16)
        return carry

    lax.fori_loop(0, n_rows // mm_rows, hidden_rows, 0)

    scale_out = (n_tp * wg.shape[1]) ** (-0.5)

    piece = n_rows // NR
    per_piece = n_fs // NR

    def ring(r):
        step = 1 - 2 * (r % 2)
        return (y + n_y + step) % n_y, (y + n_y - step) % n_y, (y + n_y // 2) % n_y

    def partial(q, r, col_tp):
        rows = pl.ds(pl.multiple_of(r * piece, piece), piece)
        cols = pl.ds(pl.multiple_of(col_tp * wide + q * wq, wq), wq)
        return jnp.dot(hidden[rows, :], wd[:, cols], preferred_element_type=F32)

    def finish(q):
        def one(r, carry):
            wait_recv(yrecv.at[q, r], ys_r.at[q, r])
            total = ysum[q, r, y].astype(F32) + yrecv[q, r, 0].astype(F32) + yrecv[q, r, 1].astype(F32)
            rsend[q, pl.ds(pl.multiple_of(r * piece, piece), piece), :] = (total * scale_out).astype(BF16)

            def give(i, carry):
                to = r * per_piece + i
                block = pl.ds(pl.multiple_of(to * cap, cap), cap)
                mine = pl.ds(pl.multiple_of(f * cap, cap), cap)

                @pl.when(to == f)
                def _():
                    rrecv[q, mine, :] = rsend[q, mine, :]

                @pl.when(to != f)
                def _():
                    remote(rsend.at[q, block, :], rrecv.at[q, mine, :], rt_s, rt_r.at[q], (g, to, t)).start()

                return carry

            lax.fori_loop(0, per_piece, give, 0)
            return carry

        lax.fori_loop(0, NR, one, 0)

    def pass_chunk(q):
        def pass_on(r, carry):
            wait_recv(passing.at[q, r], ps_y.at[q, r])
            ahead, _, _ = ring(r)
            ysum[q, r, ahead] = (ysum[q, r, ahead].astype(F32) + passing[q, r].astype(F32)).astype(BF16)
            remote(ysum.at[q, r, ahead], yrecv.at[q, r, 1], ys_s, ys_r.at[q, r], (g, f, ahead * n_c + c)).start()
            return carry

        lax.fori_loop(0, NR, pass_on, 0)

    def combine(q):
        wait_recv(rrecv.at[q, pl.ds(0, (n_fs - 1) * cap), :], rt_r.at[q])
        dn = (((0,), (0,)), ((), ()))
        got = rrecv[q]
        out = lax.dot_general(share_hi[...], got, dn, preferred_element_type=F32)
        out = out + lax.dot_general(share_lo[...], got, dn, preferred_element_type=F32)
        mixed_out[:, q * wq : (q + 1) * wq] = out.astype(BF16)

    for q in range(NQ):

        @pl.when(z == t)
        def _(q=q):
            wait_recv(wg.at[pl.ds(0, all_but_one // NQ), :], d_r.at[q])

        @pl.when(z != t)
        def _(q=q):
            wait_recv(wg.at[pl.ds(0, wg.shape[0] // NQ), :], d_r.at[q])

        def for_sibling(r, carry, q=q):
            for yy in range(n_y):
                psend[q, r, yy] = partial(q, r, yy * n_c + (1 - c)).astype(BF16)
            remote(psend.at[q, r], precv.at[q, r], ps_s, ps_r.at[q, r], sibling).start()
            return carry

        if q + 2 < NQ:
            start_down(q + 2)
        lax.fori_loop(0, NR, for_sibling, 0)

        def for_own(r, carry, q=q):
            for yy in range(n_y):
                ysum[q, r, yy] = partial(q, r, yy * n_c + c).astype(BF16)
            return carry

        lax.fori_loop(0, NR, for_own, 0)

        def exchange(r, carry, q=q):
            wait_recv(precv.at[q, r], ps_r.at[q, r])
            for yy in range(n_y):
                ysum[q, r, yy] = (ysum[q, r, yy].astype(F32) + precv[q, r, yy].astype(F32)).astype(BF16)
            ahead, behind, far = ring(r)
            remote(ysum.at[q, r, far], passing.at[q, r], ys_s, ps_y.at[q, r], (g, f, ahead * n_c + c)).start()
            remote(ysum.at[q, r, behind], yrecv.at[q, r, 0], ys_s, ys_r.at[q, r], (g, f, behind * n_c + c)).start()
            return carry

        lax.fori_loop(0, NR, exchange, 0)
        if q > 0:
            pass_chunk(q - 1)
        if q > 1:
            finish(q - 2)
        if q > 2:
            combine(q - 3)
    pass_chunk(NQ - 1)
    for q in range(max(NQ - 2, 0), NQ):
        finish(q)
    for q in range(max(NQ - 3, 0), NQ):
        combine(q)

    wait_send(slots.at[pl.ds(0, (n_fs - 1) * cap), :], disp_s)
    wait_send(wg.at[pl.ds(0, all_but_one), :], w_s.at[0])
    wait_send(wu.at[pl.ds(0, all_but_one), :], w_s.at[1])

    @pl.when(z == t)
    def _():
        wait_send(wg.at[pl.ds(0, all_but_one), :], w_s.at[2])

    @pl.when(z != t)
    def _():
        wait_send(wg, w_s.at[2])

    wait_send(psend, ps_s)
    wait_send(ysum.at[:, :, pl.ds(0, n_y - 1)], ys_s)
    wait_send(rrecv.at[:, pl.ds(0, (n_fs - 1) * cap), :], rt_s)


def write_out(*refs):
    n = len(refs) // 2
    srcs, dsts, sem = refs[:n], refs[n : 2 * n], refs[2 * n]
    copies = [pltpu.make_async_copy(src, dst, sem.at[i]) for i, (src, dst) in enumerate(zip(srcs, dsts))]
    for copy in copies:
        copy.start()
    for copy in copies:
        copy.wait()


def body(tokens, route_ids, route_logits, gain, gate_master, up_master, down_master, *, sizes):
    n_gr, n_zl, n_x, n_y, n_c = sizes
    experts, rows_g, ff = gate_master.shape
    rows_d, wide = down_master.shape[1:]
    n_tok, top = route_ids.shape
    cap = 2 * n_tok * top // experts
    n_fs, n_tp = n_zl * n_x, n_y * n_c
    n_rows = n_fs * cap
    d_model, hid = wide * n_tp, ff
    wq = wide // NQ
    vmem = lambda *shape, dtype=BF16: pltpu.VMEM(shape, dtype)
    dma = pltpu.SemaphoreType.DMA
    any_spec = pl.BlockSpec(memory_space=pl.ANY)
    vmem_spec = pl.BlockSpec(memory_space=pltpu.VMEM)
    results = pl.pallas_call(
        functools.partial(kernel, (n_gr, n_zl, n_x, n_y, n_c, cap)),
        out_shape=(
            pltpu.VMEM((1, d_model, ff), BF16),
            pltpu.VMEM((1, d_model, ff), BF16),
            pltpu.VMEM((1, hid, d_model), BF16),
            pltpu.VMEM((n_tok, wide), BF16),
        ),
        in_specs=[any_spec] * 7,
        out_specs=(vmem_spec,) * 4,
        scratch_shapes=[
            vmem(experts, rows_g, ff, dtype=F32),
            vmem(experts, rows_g, ff, dtype=F32),
            vmem(experts, rows_d, wide, dtype=F32),
            vmem(experts, rows_g, ff),
            vmem(experts, rows_g, ff),
            vmem(NQ, experts, rows_d, wq),
            vmem(n_rows, wide),
            vmem(n_rows, n_tok),
            vmem(n_rows, n_tok),
            vmem(n_tp, n_rows, wide),
            vmem(n_rows, hid, dtype=F32),
            vmem(n_rows, hid),
            vmem(n_tok, wide),
            vmem(top, n_tok, dtype=jnp.int32),
            vmem(top, n_tok, dtype=F32),
            vmem(1, rows_g, dtype=F32),
            vmem(NQ, NR, n_y, n_rows // NR, wq),
            vmem(NQ, NR, n_y, n_rows // NR, wq),
            vmem(NQ, NR, n_y, n_rows // NR, wq),
            vmem(NQ, NR, n_rows // NR, wq),
            vmem(NQ, NR, 2, n_rows // NR, wq),
            vmem(NQ, n_rows, wq),
            vmem(NQ, n_rows, wq),
            dma((7,)), dma, dma, dma((3,)), dma, dma, dma((NQ,)),
            dma, dma((n_y,)), dma, dma((n_y,)), dma, dma((NQ, NR)), dma, dma((NQ, NR)), dma((NQ, NR)), dma, dma((NQ,)),
        ],
        compiler_params=pltpu.CompilerParams(
            collective_id=0, has_side_effects=True, vmem_limit_bytes=50 * 1024 * 1024
        ),
    )(tokens, route_ids.T, route_logits.T, gain[None, :], gate_master, up_master, down_master)
    return pl.pallas_call(
        write_out,
        out_shape=tuple(jax.ShapeDtypeStruct(r.shape, r.dtype) for r in results),
        in_specs=[vmem_spec] * 4,
        out_specs=(any_spec,) * 4,
        scratch_shapes=[dma((4,))],
        compiler_params=pltpu.CompilerParams(vmem_limit_bytes=1024 * 1024),
    )(*(pltpu.with_memory_space_constraint(r, pltpu.VMEM) for r in results))


def solution(mesh):
    n_zl, n_x, n_c = 4, 4, 2
    sizes = (mesh.shape["gr"], n_zl, n_x, mesh.shape["tp"] // n_c, n_c)
    in_specs = (
        P(("gr", "fs"), "tp"),
        P(("gr", "fs"), None),
        P(("gr", "fs"), None),
        P(("gr", "fs")),
        P(None, ("gr", "fs"), "tp"),
        P(None, ("gr", "fs"), "tp"),
        P(None, ("gr", "fs"), "tp"),
    )
    out_specs = (
        P("fs", None, "tp"),
        P("fs", None, "tp"),
        P("fs", "tp", None),
        P(("gr", "fs"), "tp"),
    )
    return jax.shard_map(
        functools.partial(body, sizes=sizes), mesh=mesh, in_specs=in_specs, out_specs=out_specs, check_vma=False
    )
```

```python
import functools

import jax
import jax.numpy as jnp
from jax import lax
from jax.experimental import pallas as pl
from jax.experimental.pallas import tpu as pltpu
from jax.sharding import PartitionSpec as P

EPS = 1e-06
MESH = pl.DeviceIdType.MESH
F32 = jnp.float32
BF16 = jnp.bfloat16
NQ = 4
NR = 4


def kernel(
    dims,
    tok_hbm, ids_hbm, logit_hbm, gain_hbm, gate_hbm, up_hbm, down_hbm,
    wg_out, wu_out, wd_out, mixed_out,
    stage_g, stage_u, stage_d, snd_g, snd_u, snd_d,
    slots, share_hi, share_lo, xall, gate_act, hidden,
    tok_ref, ids_ref, logit_ref, gain_ref,
    psend, precv, ysum, passing, yrecv, rsend, rrecv,
    load_sem, disp_s, disp_r, w_s, g_r, u_r, d_r,
    ag_s, ag_r, sib_s, sib_r, ps_s, ps_r, ys_s, ps_y, ys_r, rt_s, rt_r,
):
    n_gr, n_zl, n_x, n_y, n_c, cap = dims
    wg, wu, wd = wg_out.at[0], wu_out.at[0], wd_out.at[0]
    n_fs = n_zl * n_x
    n_z = n_gr * n_zl
    n_tp = n_y * n_c
    g = lax.axis_index("gr")
    f = lax.axis_index("fs")
    t = lax.axis_index("tp")
    z = g * n_zl + f // n_x
    x = f % n_x
    y = t // n_c
    c = t % n_c
    part = g * n_fs + f
    rows_g = stage_g.shape[1]
    rows_d = stage_d.shape[1]
    wide = tok_ref.shape[1]
    wq = wide // NQ
    n_rows = n_fs * cap
    n_peer = n_z * n_x
    d_model = n_tp * wide
    half = rows_g // 2
    sibling = (g, f, y * n_c + (1 - c))

    def remote(src, dst, s_sem, r_sem, to):
        return pltpu.make_async_remote_copy(
            src_ref=src, dst_ref=dst, send_sem=s_sem, recv_sem=r_sem, device_id=to, device_id_type=MESH
        )

    def wait_recv(ref, sem):
        remote(ref, ref, sem, sem, sibling).wait_recv()

    def wait_send(ref, sem):
        remote(ref, ref, sem, sem, sibling).wait_send()

    def peer(i, turn=0):
        a = i % n_z
        off = n_z // 2 + (1 - 2 * (a % 2)) * ((a + 1) // 2)
        zz = (z + off) % n_z
        xx = (x + 1 + i // n_z + turn) % n_x
        return zz // n_zl, (zz % n_zl) * n_x + xx

    barrier = pltpu.get_barrier_semaphore()

    def greet(i, carry):
        pg, pf = peer(i)
        pl.semaphore_signal(barrier, inc=1, device_id=(pg, pf, t), device_id_type=MESH)
        return carry


    def greet_down(i, carry):
        to = (t // n_zl, (t % n_zl) * n_x + i // n_tp, i % n_tp)
        mine = jnp.logical_and(z == t, jnp.logical_and(i // n_tp == x, i % n_tp == t))

        @pl.when(jnp.logical_not(mine))
        def _():
            pl.semaphore_signal(barrier, inc=1, device_id=to, device_id_type=MESH)

        return carry

    lax.fori_loop(0, n_x * n_tp, greet_down, 0, unroll=True)
    lax.fori_loop(0, n_peer - 1, greet, 0, unroll=True)
    for dy in range(1, n_y):
        pl.semaphore_signal(barrier, inc=1, device_id=(g, f, ((y + dy) % n_y) * n_c + c), device_id_type=MESH)
    pl.semaphore_signal(barrier, inc=1, device_id=sibling, device_id_type=MESH)

    loads = [
        pltpu.make_async_copy(gate_hbm, stage_g, load_sem.at[0]),
        pltpu.make_async_copy(up_hbm, stage_u, load_sem.at[1]),
        pltpu.make_async_copy(down_hbm, stage_d, load_sem.at[2]),
    ]
    small = [
        pltpu.make_async_copy(src, dst, load_sem.at[3 + i])
        for i, (src, dst) in enumerate(
            ((tok_hbm, tok_ref), (ids_hbm, ids_ref), (logit_hbm, logit_ref), (gain_hbm, gain_ref))
        )
    ]
    for copy in small + loads:
        copy.start()

    for copy in small:
        copy.wait()
    n_tok = tok_ref.shape[0]
    ids = ids_ref[...]
    sig = jax.nn.sigmoid(logit_ref[...])
    share = sig / jnp.sum(sig, axis=0, keepdims=True)
    experts = lax.broadcasted_iota(jnp.int32, (n_fs, n_tok), 0)
    hit0 = (ids[0:1, :] == experts).astype(F32)
    hit1 = (ids[1:2, :] == experts).astype(F32)
    member = hit0 + hit1
    weight = hit0 * share[0:1, :] + hit1 * share[1:2, :]
    earlier = (
        lax.broadcasted_iota(jnp.int32, (n_tok, n_tok), 0) < lax.broadcasted_iota(jnp.int32, (n_tok, n_tok), 1)
    ).astype(BF16)
    rank = jnp.dot(member.astype(BF16), earlier, preferred_element_type=F32)
    rank = jnp.where(member > 0.5, rank, -1.0)
    slot_no = lax.broadcasted_iota(jnp.int32, (cap, n_tok), 0).astype(F32)
    tok = tok_ref[...]
    for e in range(n_fs):
        pick = (slot_no == rank[e : e + 1, :]).astype(F32)
        slots[e * cap : (e + 1) * cap, :] = jnp.dot(
            pick.astype(BF16), tok, preferred_element_type=F32
        ).astype(BF16)
        scaled = pick * weight[e : e + 1, :]
        hi = scaled.astype(BF16)
        share_hi[e * cap : (e + 1) * cap, :] = hi
        share_lo[e * cap : (e + 1) * cap, :] = (scaled - hi.astype(F32)).astype(BF16)

    gcol = jnp.broadcast_to(gain_ref[...], (rows_g, rows_g)).T
    loads[0].wait()

    def cast_gate(e, carry):
        for h in range(0, stage_g.shape[2], rows_g):
            snd_g[e, :, h : h + rows_g] = (stage_g[e, :, h : h + rows_g] * gcol).astype(BF16)
        return carry

    lax.fori_loop(0, n_fs, cast_gate, 0)
    wg[pl.ds(pl.multiple_of(part * rows_g, rows_g), rows_g), :] = snd_g[f]
    loads[1].wait()

    def cast_up(e, carry):
        for h in range(0, stage_u.shape[2], rows_g):
            snd_u[e, :, h : h + rows_g] = (stage_u[e, :, h : h + rows_g] * gcol).astype(BF16)
        return carry

    lax.fori_loop(0, n_fs, cast_up, 0)
    wu[pl.ds(pl.multiple_of(part * rows_g, rows_g), rows_g), :] = snd_u[f]
    loads[2].wait()

    def cast_down(e, carry):
        for q in range(NQ):
            snd_d[q, e] = stage_d[e, :, q * wq : (q + 1) * wq].astype(BF16)
        return carry

    lax.fori_loop(0, n_fs, cast_down, 0)

    def down_place(q):
        return wd.at[
            pl.ds(pl.multiple_of(x * rows_d, rows_d), rows_d),
            pl.ds(pl.multiple_of(t * wide + q * wq, wq), wq),
        ]

    @pl.when(z == t)
    def _():
        for q in range(NQ):
            wd[
                pl.ds(pl.multiple_of(x * rows_d, rows_d), rows_d),
                pl.ds(pl.multiple_of(t * wide + q * wq, wq), wq),
            ] = snd_d[q, f]

    mine_x = xall.at[t, pl.ds(pl.multiple_of(f * cap, cap), cap), :]
    xall[t, pl.ds(pl.multiple_of(f * cap, cap), cap), :] = slots[pl.ds(pl.multiple_of(f * cap, cap), cap), :]

    pl.semaphore_wait(barrier, (n_peer - 1) + (n_y - 1) + 1 + n_peer - jnp.where(z == t, 1, 0))

    def dispatch(i, carry):
        a = i % n_zl
        off = n_zl // 2 + (2 * (a % 2) - 1) * ((a + 1) // 2)
        to = (f // n_x + off) % n_zl * n_x + (x + 1 + i // n_zl) % n_x
        remote(
            slots.at[pl.ds(pl.multiple_of(to * cap, cap), cap), :], mine_x, disp_s, disp_r, (g, to, t)
        ).start()
        return carry

    lax.fori_loop(0, n_fs - 1, dispatch, 0)

    def send_gate(i, carry):
        pg, pf = peer(i % (n_peer - 1))
        first = pl.multiple_of(i // (n_peer - 1) * half, half)
        remote(
            snd_g.at[pf, pl.ds(first, half), :],
            wg.at[pl.ds(pl.multiple_of(part * rows_g + first, half), half), :],
            w_s.at[0], g_r, (pg, pf, t),
        ).start()
        return carry

    lax.fori_loop(0, 2 * (n_peer - 1), send_gate, 0)

    wait_recv(xall.at[0, pl.ds(0, (n_fs - 1) * cap), :], disp_r)
    for dy in range(1, n_y):
        remote(xall.at[t], xall.at[t], ag_s, ag_r.at[n_y - dy], (g, f, ((y + dy) % n_y) * n_c + c)).start()
    remote(xall.at[t], xall.at[t], sib_s, sib_r.at[0], sibling).start()

    def send_up(i, carry):
        pg, pf = peer(i % (n_peer - 1))
        first = pl.multiple_of(i // (n_peer - 1) * half, half)
        remote(
            snd_u.at[pf, pl.ds(first, half), :],
            wu.at[pl.ds(pl.multiple_of(part * rows_g + first, half), half), :],
            w_s.at[1], u_r, (pg, pf, t),
        ).start()
        return carry

    lax.fori_loop(0, 2 * (n_peer - 1), send_up, 0)
    for dy in range(1, n_y):
        from_tp = ((y + dy) % n_y) * n_c + c
        wait_recv(xall.at[from_tp], ag_r.at[dy])
        remote(xall.at[from_tp], xall.at[from_tp], sib_s, sib_r.at[dy], sibling).start()
    for dy in range(n_y):
        from_tp = ((y + dy) % n_y) * n_c + (1 - c)
        wait_recv(xall.at[from_tp], sib_r.at[dy])
    wait_send(xall.at[pl.ds(0, n_y - 1)], ag_s)
    wait_send(xall.at[pl.ds(0, n_y)], sib_s)

    row_block = 32

    def normalize(i, carry):
        rows = pl.ds(pl.multiple_of(i * row_block, row_block), row_block)
        squares = jnp.zeros((row_block, wide), F32)
        for k in range(n_tp):
            v = xall[k, rows, :].astype(F32)
            squares = squares + v * v
        scale = lax.rsqrt(jnp.sum(squares, axis=1, keepdims=True) / d_model + EPS)
        for k in range(n_tp):
            xall[k, rows, :] = (xall[k, rows, :].astype(F32) * scale).astype(BF16)
        return carry

    lax.fori_loop(0, n_rows // row_block, normalize, 0)

    def start_down(q):
        def send_down(i, carry):
            pg, pf = peer(i, y)
            here = jnp.logical_and(jnp.logical_and(pg == g, pf == f), t == z)

            @pl.when(jnp.logical_not(here))
            def _():
                remote(snd_d.at[q, pf], down_place(q), w_s.at[2], d_r.at[q], (pg, pf, z)).start()

            return carry

        lax.fori_loop(0, n_peer, send_down, 0)

    for q in range(2):
        start_down(q)

    all_but_one = (n_peer - 1) * rows_g
    wait_recv(wg.at[pl.ds(0, all_but_one), :], g_r)
    scale_in = d_model ** (-0.5)
    mm_rows = 256

    def product(w, rows):
        total = jnp.zeros((mm_rows, w.shape[1]), F32)
        for k in range(n_tp):
            total = total + jnp.dot(xall[k, rows, :], w[k * wide : (k + 1) * wide, :], preferred_element_type=F32)
        return total * scale_in

    def gate_rows(i, carry):
        rows = pl.ds(pl.multiple_of(i * mm_rows, mm_rows), mm_rows)
        gate_value = product(wg, rows)
        gate_act[rows, :] = gate_value * jax.nn.sigmoid(gate_value)
        return carry

    lax.fori_loop(0, n_rows // mm_rows, gate_rows, 0)
    wait_recv(wu.at[pl.ds(0, all_but_one), :], u_r)

    def hidden_rows(i, carry):
        rows = pl.ds(pl.multiple_of(i * mm_rows, mm_rows), mm_rows)
        hidden[rows, :] = (gate_act[rows, :] * product(wu, rows)).astype(BF16)
        return carry

    lax.fori_loop(0, n_rows // mm_rows, hidden_rows, 0)

    scale_out = (n_tp * wg.shape[1]) ** (-0.5)

    piece = n_rows // NR
    per_piece = n_fs // NR

    def ring(r):
        step = 1 - 2 * (r % 2)
        return (y + n_y + step) % n_y, (y + n_y - step) % n_y, (y + n_y // 2) % n_y

    def partial(q, r, col_tp):
        rows = pl.ds(pl.multiple_of(r * piece, piece), piece)
        cols = pl.ds(pl.multiple_of(col_tp * wide + q * wq, wq), wq)
        return jnp.dot(hidden[rows, :], wd[:, cols], preferred_element_type=F32)

    def finish(q):
        def one(r, carry):
            wait_recv(yrecv.at[q, r], ys_r.at[q, r])
            total = ysum[q, r, y].astype(F32) + yrecv[q, r, 0].astype(F32) + yrecv[q, r, 1].astype(F32)
            rsend[q, pl.ds(pl.multiple_of(r * piece, piece), piece), :] = (total * scale_out).astype(BF16)

            def give(i, carry):
                to = r * per_piece + i
                block = pl.ds(pl.multiple_of(to * cap, cap), cap)
                mine = pl.ds(pl.multiple_of(f * cap, cap), cap)

                @pl.when(to == f)
                def _():
                    rrecv[q, mine, :] = rsend[q, mine, :]

                @pl.when(to != f)
                def _():
                    remote(rsend.at[q, block, :], rrecv.at[q, mine, :], rt_s, rt_r.at[q], (g, to, t)).start()

                return carry

            lax.fori_loop(0, per_piece, give, 0)
            return carry

        lax.fori_loop(0, NR, one, 0)

    def pass_chunk(q):
        def pass_on(r, carry):
            wait_recv(passing.at[q, r], ps_y.at[q, r])
            ahead, _, _ = ring(r)
            ysum[q, r, ahead] = (ysum[q, r, ahead].astype(F32) + passing[q, r].astype(F32)).astype(BF16)
            remote(ysum.at[q, r, ahead], yrecv.at[q, r, 1], ys_s, ys_r.at[q, r], (g, f, ahead * n_c + c)).start()
            return carry

        lax.fori_loop(0, NR, pass_on, 0)

    def combine(q):
        wait_recv(rrecv.at[q, pl.ds(0, (n_fs - 1) * cap), :], rt_r.at[q])
        dn = (((0,), (0,)), ((), ()))
        got = rrecv[q]
        out = lax.dot_general(share_hi[...], got, dn, preferred_element_type=F32)
        out = out + lax.dot_general(share_lo[...], got, dn, preferred_element_type=F32)
        mixed_out[:, q * wq : (q + 1) * wq] = out.astype(BF16)

    for q in range(NQ):

        @pl.when(z == t)
        def _(q=q):
            wait_recv(wg.at[pl.ds(0, all_but_one // NQ), :], d_r.at[q])

        @pl.when(z != t)
        def _(q=q):
            wait_recv(wg.at[pl.ds(0, wg.shape[0] // NQ), :], d_r.at[q])

        def for_sibling(r, carry, q=q):
            for yy in range(n_y):
                psend[q, r, yy] = partial(q, r, yy * n_c + (1 - c)).astype(BF16)
            remote(psend.at[q, r], precv.at[q, r], ps_s, ps_r.at[q, r], sibling).start()
            return carry

        if q + 2 < NQ:
            start_down(q + 2)
        lax.fori_loop(0, NR, for_sibling, 0)

        def for_own(r, carry, q=q):
            for yy in range(n_y):
                ysum[q, r, yy] = partial(q, r, yy * n_c + c).astype(BF16)
            return carry

        lax.fori_loop(0, NR, for_own, 0)

        def exchange(r, carry, q=q):
            wait_recv(precv.at[q, r], ps_r.at[q, r])
            for yy in range(n_y):
                ysum[q, r, yy] = (ysum[q, r, yy].astype(F32) + precv[q, r, yy].astype(F32)).astype(BF16)
            ahead, behind, far = ring(r)
            remote(ysum.at[q, r, far], passing.at[q, r], ys_s, ps_y.at[q, r], (g, f, ahead * n_c + c)).start()
            remote(ysum.at[q, r, behind], yrecv.at[q, r, 0], ys_s, ys_r.at[q, r], (g, f, behind * n_c + c)).start()
            return carry

        lax.fori_loop(0, NR, exchange, 0)
        if q > 0:
            pass_chunk(q - 1)
        if q > 1:
            finish(q - 2)
        if q > 2:
            combine(q - 3)
    pass_chunk(NQ - 1)
    for q in range(max(NQ - 2, 0), NQ):
        finish(q)
    for q in range(max(NQ - 3, 0), NQ):
        combine(q)

    wait_send(slots.at[pl.ds(0, (n_fs - 1) * cap), :], disp_s)
    wait_send(wg.at[pl.ds(0, all_but_one), :], w_s.at[0])
    wait_send(wu.at[pl.ds(0, all_but_one), :], w_s.at[1])

    @pl.when(z == t)
    def _():
        wait_send(wg.at[pl.ds(0, all_but_one), :], w_s.at[2])

    @pl.when(z != t)
    def _():
        wait_send(wg, w_s.at[2])

    wait_send(psend, ps_s)
    wait_send(ysum.at[:, :, pl.ds(0, n_y - 1)], ys_s)
    wait_send(rrecv.at[:, pl.ds(0, (n_fs - 1) * cap), :], rt_s)


def write_out(*refs):
    n = len(refs) // 2
    sem = refs[2 * n]
    copies = []
    for i, (src, dst) in enumerate(zip(refs[:n], refs[n : 2 * n])):
        parts = 4 if len(src.shape) == 3 else 1
        size = src.shape[-2] // parts
        for p in range(parts):
            rows = (slice(None),) * (len(src.shape) - 2) + (pl.ds(p * size, size),)
            copies.append(pltpu.make_async_copy(src.at[rows], dst.at[rows], sem.at[i, p]))
    for copy in copies:
        copy.start()
    for copy in copies:
        copy.wait()


def body(tokens, route_ids, route_logits, gain, gate_master, up_master, down_master, *, sizes):
    n_gr, n_zl, n_x, n_y, n_c = sizes
    experts, rows_g, ff = gate_master.shape
    rows_d, wide = down_master.shape[1:]
    n_tok, top = route_ids.shape
    cap = 2 * n_tok * top // experts
    n_fs, n_tp = n_zl * n_x, n_y * n_c
    n_rows = n_fs * cap
    d_model, hid = wide * n_tp, ff
    wq = wide // NQ
    vmem = lambda *shape, dtype=BF16: pltpu.VMEM(shape, dtype)
    dma = pltpu.SemaphoreType.DMA
    any_spec = pl.BlockSpec(memory_space=pl.ANY)
    vmem_spec = pl.BlockSpec(memory_space=pltpu.VMEM)
    results = pl.pallas_call(
        functools.partial(kernel, (n_gr, n_zl, n_x, n_y, n_c, cap)),
        out_shape=(
            pltpu.VMEM((1, d_model, ff), BF16),
            pltpu.VMEM((1, d_model, ff), BF16),
            pltpu.VMEM((1, hid, d_model), BF16),
            pltpu.VMEM((n_tok, wide), BF16),
        ),
        in_specs=[any_spec] * 7,
        out_specs=(vmem_spec,) * 4,
        scratch_shapes=[
            vmem(experts, rows_g, ff, dtype=F32),
            vmem(experts, rows_g, ff, dtype=F32),
            vmem(experts, rows_d, wide, dtype=F32),
            vmem(experts, rows_g, ff),
            vmem(experts, rows_g, ff),
            vmem(NQ, experts, rows_d, wq),
            vmem(n_rows, wide),
            vmem(n_rows, n_tok),
            vmem(n_rows, n_tok),
            vmem(n_tp, n_rows, wide),
            vmem(n_rows, hid, dtype=F32),
            vmem(n_rows, hid),
            vmem(n_tok, wide),
            vmem(top, n_tok, dtype=jnp.int32),
            vmem(top, n_tok, dtype=F32),
            vmem(1, rows_g, dtype=F32),
            vmem(NQ, NR, n_y, n_rows // NR, wq),
            vmem(NQ, NR, n_y, n_rows // NR, wq),
            vmem(NQ, NR, n_y, n_rows // NR, wq),
            vmem(NQ, NR, n_rows // NR, wq),
            vmem(NQ, NR, 2, n_rows // NR, wq),
            vmem(NQ, n_rows, wq),
            vmem(NQ, n_rows, wq),
            dma((7,)), dma, dma, dma((3,)), dma, dma, dma((NQ,)),
            dma, dma((n_y,)), dma, dma((n_y,)), dma, dma((NQ, NR)), dma, dma((NQ, NR)), dma((NQ, NR)), dma, dma((NQ,)),
        ],
        compiler_params=pltpu.CompilerParams(
            collective_id=0, has_side_effects=True, vmem_limit_bytes=50 * 1024 * 1024
        ),
    )(tokens, route_ids.T, route_logits.T, gain[None, :], gate_master, up_master, down_master)
    return pl.pallas_call(
        write_out,
        out_shape=tuple(jax.ShapeDtypeStruct(r.shape, r.dtype) for r in results),
        in_specs=[vmem_spec] * 4,
        out_specs=(any_spec,) * 4,
        scratch_shapes=[dma((4, 4))],
        compiler_params=pltpu.CompilerParams(vmem_limit_bytes=1024 * 1024),
    )(*(pltpu.with_memory_space_constraint(r, pltpu.VMEM) for r in results))


def solution(mesh):
    n_zl, n_x, n_c = 4, 4, 2
    sizes = (mesh.shape["gr"], n_zl, n_x, mesh.shape["tp"] // n_c, n_c)
    in_specs = (
        P(("gr", "fs"), "tp"),
        P(("gr", "fs"), None),
        P(("gr", "fs"), None),
        P(("gr", "fs")),
        P(None, ("gr", "fs"), "tp"),
        P(None, ("gr", "fs"), "tp"),
        P(None, ("gr", "fs"), "tp"),
    )
    out_specs = (
        P("fs", None, "tp"),
        P("fs", None, "tp"),
        P("fs", "tp", None),
        P(("gr", "fs"), "tp"),
    )
    return jax.shard_map(
        functools.partial(body, sizes=sizes), mesh=mesh, in_specs=in_specs, out_specs=out_specs, check_vma=False
    )
```

```python
import functools

import jax
import jax.numpy as jnp
from jax import lax
from jax.experimental import pallas as pl
from jax.experimental.pallas import tpu as pltpu
from jax.sharding import PartitionSpec as P

EPS = 1e-06
MESH = pl.DeviceIdType.MESH
F32 = jnp.float32
BF16 = jnp.bfloat16
NQ = 4
NR = 4


def kernel(
    dims,
    tok_hbm, ids_hbm, logit_hbm, gain_hbm, gate_hbm, up_hbm, down_hbm,
    wg_out, wu_out, wd_out, mixed_out,
    stage_g, stage_u, stage_d, snd_g, snd_u, snd_d,
    slots, share_hi, share_lo, xall, gate_act, hidden,
    tok_ref, ids_ref, logit_ref, gain_ref,
    psend, precv, ysum, passing, yrecv, rsend, rrecv,
    load_sem, disp_s, disp_r, w_s, g_r, u_r, d_r,
    ag_s, ag_r, sib_s, sib_r, ps_s, ps_r, ys_s, ps_y, ys_r, rt_s, rt_r,
):
    n_gr, n_zl, n_x, n_y, n_c, cap = dims
    wg, wu, wd = wg_out.at[0], wu_out.at[0], wd_out.at[0]
    n_fs = n_zl * n_x
    n_z = n_gr * n_zl
    n_tp = n_y * n_c
    g = lax.axis_index("gr")
    f = lax.axis_index("fs")
    t = lax.axis_index("tp")
    z = g * n_zl + f // n_x
    x = f % n_x
    y = t // n_c
    c = t % n_c
    part = g * n_fs + f
    rows_g = stage_g.shape[1]
    rows_d = stage_d.shape[1]
    wide = tok_ref.shape[1]
    wq = wide // NQ
    n_rows = n_fs * cap
    n_peer = n_z * n_x
    d_model = n_tp * wide
    half = rows_g // 2
    sibling = (g, f, y * n_c + (1 - c))

    def remote(src, dst, s_sem, r_sem, to):
        return pltpu.make_async_remote_copy(
            src_ref=src, dst_ref=dst, send_sem=s_sem, recv_sem=r_sem, device_id=to, device_id_type=MESH
        )

    def wait_recv(ref, sem):
        remote(ref, ref, sem, sem, sibling).wait_recv()

    def wait_send(ref, sem):
        remote(ref, ref, sem, sem, sibling).wait_send()

    def peer(i, turn=0):
        a = i % n_z
        off = n_z // 2 + (1 - 2 * (a % 2)) * ((a + 1) // 2)
        zz = (z + off) % n_z
        xx = (x + 1 + i // n_z + turn) % n_x
        return zz // n_zl, (zz % n_zl) * n_x + xx

    barrier = pltpu.get_barrier_semaphore()

    def greet(i, carry):
        pg, pf = peer(i)
        pl.semaphore_signal(barrier, inc=1, device_id=(pg, pf, t), device_id_type=MESH)
        return carry


    def greet_down(i, carry):
        to = (t // n_zl, (t % n_zl) * n_x + i // n_tp, i % n_tp)
        mine = jnp.logical_and(z == t, jnp.logical_and(i // n_tp == x, i % n_tp == t))

        @pl.when(jnp.logical_not(mine))
        def _():
            pl.semaphore_signal(barrier, inc=1, device_id=to, device_id_type=MESH)

        return carry

    lax.fori_loop(0, n_x * n_tp, greet_down, 0, unroll=True)
    lax.fori_loop(0, n_peer - 1, greet, 0, unroll=True)
    for dy in range(1, n_y):
        pl.semaphore_signal(barrier, inc=1, device_id=(g, f, ((y + dy) % n_y) * n_c + c), device_id_type=MESH)
    pl.semaphore_signal(barrier, inc=1, device_id=sibling, device_id_type=MESH)

    loads = [
        pltpu.make_async_copy(gate_hbm, stage_g, load_sem.at[0]),
        pltpu.make_async_copy(up_hbm, stage_u, load_sem.at[1]),
        pltpu.make_async_copy(down_hbm, stage_d, load_sem.at[2]),
    ]
    small = [
        pltpu.make_async_copy(src, dst, load_sem.at[3 + i])
        for i, (src, dst) in enumerate(
            ((tok_hbm, tok_ref), (ids_hbm, ids_ref), (logit_hbm, logit_ref), (gain_hbm, gain_ref))
        )
    ]
    for copy in small + loads:
        copy.start()

    for copy in small:
        copy.wait()
    n_tok = tok_ref.shape[0]
    ids = ids_ref[...]
    sig = jax.nn.sigmoid(logit_ref[...])
    share = sig / jnp.sum(sig, axis=0, keepdims=True)
    experts = lax.broadcasted_iota(jnp.int32, (n_fs, n_tok), 0)
    hit0 = (ids[0:1, :] == experts).astype(F32)
    hit1 = (ids[1:2, :] == experts).astype(F32)
    member = hit0 + hit1
    weight = hit0 * share[0:1, :] + hit1 * share[1:2, :]
    earlier = (
        lax.broadcasted_iota(jnp.int32, (n_tok, n_tok), 0) < lax.broadcasted_iota(jnp.int32, (n_tok, n_tok), 1)
    ).astype(BF16)
    rank = jnp.dot(member.astype(BF16), earlier, preferred_element_type=F32)
    rank = jnp.where(member > 0.5, rank, -1.0)
    slot_no = lax.broadcasted_iota(jnp.int32, (cap, n_tok), 0).astype(F32)
    tok = tok_ref[...]
    for e in range(n_fs):
        pick = (slot_no == rank[e : e + 1, :]).astype(F32)
        slots[e * cap : (e + 1) * cap, :] = jnp.dot(
            pick.astype(BF16), tok, preferred_element_type=F32
        ).astype(BF16)
        scaled = pick * weight[e : e + 1, :]
        hi = scaled.astype(BF16)
        share_hi[e * cap : (e + 1) * cap, :] = hi
        share_lo[e * cap : (e + 1) * cap, :] = (scaled - hi.astype(F32)).astype(BF16)

    gcol = jnp.broadcast_to(gain_ref[...], (rows_g, rows_g)).T
    loads[0].wait()

    def cast_gate(e, carry):
        for h in range(0, stage_g.shape[2], rows_g):
            snd_g[e, :, h : h + rows_g] = (stage_g[e, :, h : h + rows_g] * gcol).astype(BF16)
        return carry

    lax.fori_loop(0, n_fs, cast_gate, 0)
    wg[pl.ds(pl.multiple_of(part * rows_g, rows_g), rows_g), :] = snd_g[f]
    loads[1].wait()

    def cast_up(e, carry):
        for h in range(0, stage_u.shape[2], rows_g):
            snd_u[e, :, h : h + rows_g] = (stage_u[e, :, h : h + rows_g] * gcol).astype(BF16)
        return carry

    lax.fori_loop(0, n_fs, cast_up, 0)
    wu[pl.ds(pl.multiple_of(part * rows_g, rows_g), rows_g), :] = snd_u[f]
    loads[2].wait()

    def cast_down(e, carry):
        for q in range(NQ):
            snd_d[q, e] = stage_d[e, :, q * wq : (q + 1) * wq].astype(BF16)
        return carry

    lax.fori_loop(0, n_fs, cast_down, 0)

    def down_place(q):
        return wd.at[
            pl.ds(pl.multiple_of(x * rows_d, rows_d), rows_d),
            pl.ds(pl.multiple_of(t * wide + q * wq, wq), wq),
        ]

    @pl.when(z == t)
    def _():
        for q in range(NQ):
            wd[
                pl.ds(pl.multiple_of(x * rows_d, rows_d), rows_d),
                pl.ds(pl.multiple_of(t * wide + q * wq, wq), wq),
            ] = snd_d[q, f]

    mine_x = xall.at[t, pl.ds(pl.multiple_of(f * cap, cap), cap), :]
    xall[t, pl.ds(pl.multiple_of(f * cap, cap), cap), :] = slots[pl.ds(pl.multiple_of(f * cap, cap), cap), :]

    pl.semaphore_wait(barrier, (n_peer - 1) + (n_y - 1) + 1 + n_peer - jnp.where(z == t, 1, 0))

    def dispatch(i, carry):
        a = i % n_zl
        off = n_zl // 2 + (2 * (a % 2) - 1) * ((a + 1) // 2)
        to = (f // n_x + off) % n_zl * n_x + (x + 1 + i // n_zl) % n_x
        remote(
            slots.at[pl.ds(pl.multiple_of(to * cap, cap), cap), :], mine_x, disp_s, disp_r, (g, to, t)
        ).start()
        return carry

    lax.fori_loop(0, n_fs - 1, dispatch, 0)

    def send_gate(i, carry):
        pg, pf = peer(i % (n_peer - 1))
        first = pl.multiple_of(i // (n_peer - 1) * half, half)
        remote(
            snd_g.at[pf, pl.ds(first, half), :],
            wg.at[pl.ds(pl.multiple_of(part * rows_g + first, half), half), :],
            w_s.at[0], g_r, (pg, pf, t),
        ).start()
        return carry

    lax.fori_loop(0, 2 * (n_peer - 1), send_gate, 0)

    wait_recv(xall.at[0, pl.ds(0, (n_fs - 1) * cap), :], disp_r)
    for dy in range(1, n_y):
        remote(xall.at[t], xall.at[t], ag_s, ag_r.at[n_y - dy], (g, f, ((y + dy) % n_y) * n_c + c)).start()
    remote(xall.at[t], xall.at[t], sib_s, sib_r.at[0], sibling).start()

    def send_up(i, carry):
        pg, pf = peer(i % (n_peer - 1))
        first = pl.multiple_of(i // (n_peer - 1) * half, half)
        remote(
            snd_u.at[pf, pl.ds(first, half), :],
            wu.at[pl.ds(pl.multiple_of(part * rows_g + first, half), half), :],
            w_s.at[1], u_r, (pg, pf, t),
        ).start()
        return carry

    lax.fori_loop(0, 2 * (n_peer - 1), send_up, 0)
    for dy in range(1, n_y):
        from_tp = ((y + dy) % n_y) * n_c + c
        wait_recv(xall.at[from_tp], ag_r.at[dy])
        remote(xall.at[from_tp], xall.at[from_tp], sib_s, sib_r.at[dy], sibling).start()
    for dy in range(n_y):
        from_tp = ((y + dy) % n_y) * n_c + (1 - c)
        wait_recv(xall.at[from_tp], sib_r.at[dy])
    wait_send(xall.at[pl.ds(0, n_y - 1)], ag_s)
    wait_send(xall.at[pl.ds(0, n_y)], sib_s)

    row_block = 32

    def normalize(i, carry):
        rows = pl.ds(pl.multiple_of(i * row_block, row_block), row_block)
        squares = jnp.zeros((row_block, wide), F32)
        for k in range(n_tp):
            v = xall[k, rows, :].astype(F32)
            squares = squares + v * v
        scale = lax.rsqrt(jnp.sum(squares, axis=1, keepdims=True) / d_model + EPS)
        for k in range(n_tp):
            xall[k, rows, :] = (xall[k, rows, :].astype(F32) * scale).astype(BF16)
        return carry

    lax.fori_loop(0, n_rows // row_block, normalize, 0)

    def start_down(q):
        def send_down(i, carry):
            pg, pf = peer(i, y)
            here = jnp.logical_and(jnp.logical_and(pg == g, pf == f), t == z)

            @pl.when(jnp.logical_not(here))
            def _():
                remote(snd_d.at[q, pf], down_place(q), w_s.at[2], d_r.at[q], (pg, pf, z)).start()

            return carry

        lax.fori_loop(0, n_peer, send_down, 0)

    for q in range(2):
        start_down(q)

    all_but_one = (n_peer - 1) * rows_g
    wait_recv(wg.at[pl.ds(0, all_but_one), :], g_r)
    scale_in = d_model ** (-0.5)
    mm_rows = 256

    def product(w, rows):
        total = jnp.zeros((mm_rows, w.shape[1]), F32)
        for k in range(n_tp):
            total = total + jnp.dot(xall[k, rows, :], w[k * wide : (k + 1) * wide, :], preferred_element_type=F32)
        return total * scale_in

    def gate_rows(i, carry):
        rows = pl.ds(pl.multiple_of(i * mm_rows, mm_rows), mm_rows)
        gate_value = product(wg, rows)
        gate_act[rows, :] = gate_value * jax.nn.sigmoid(gate_value)
        return carry

    lax.fori_loop(0, n_rows // mm_rows, gate_rows, 0)
    wait_recv(wu.at[pl.ds(0, all_but_one), :], u_r)

    def hidden_rows(i, carry):
        rows = pl.ds(pl.multiple_of(i * mm_rows, mm_rows), mm_rows)
        hidden[rows, :] = (gate_act[rows, :] * product(wu, rows)).astype(BF16)
        return carry

    lax.fori_loop(0, n_rows // mm_rows, hidden_rows, 0)

    scale_out = (n_tp * wg.shape[1]) ** (-0.5)

    piece = n_rows // NR
    per_piece = n_fs // NR

    def ring(r):
        step = 1 - 2 * (r % 2)
        return (y + n_y + step) % n_y, (y + n_y - step) % n_y, (y + n_y // 2) % n_y

    def partial(q, r, col_tp):
        rows = pl.ds(pl.multiple_of(r * piece, piece), piece)
        cols = pl.ds(pl.multiple_of(col_tp * wide + q * wq, wq), wq)
        return jnp.dot(hidden[rows, :], wd[:, cols], preferred_element_type=F32)

    def finish(q):
        def one(r, carry):
            wait_recv(yrecv.at[q, r], ys_r.at[q, r])
            total = ysum[q, r, y].astype(F32) + yrecv[q, r, 0].astype(F32) + yrecv[q, r, 1].astype(F32)
            rsend[q, pl.ds(pl.multiple_of(r * piece, piece), piece), :] = (total * scale_out).astype(BF16)

            def give(i, carry):
                to = r * per_piece + i
                block = pl.ds(pl.multiple_of(to * cap, cap), cap)
                mine = pl.ds(pl.multiple_of(f * cap, cap), cap)

                @pl.when(to == f)
                def _():
                    rrecv[q, mine, :] = rsend[q, mine, :]

                @pl.when(to != f)
                def _():
                    remote(rsend.at[q, block, :], rrecv.at[q, mine, :], rt_s, rt_r.at[q], (g, to, t)).start()

                return carry

            lax.fori_loop(0, per_piece, give, 0)
            return carry

        lax.fori_loop(0, NR, one, 0)

    def pass_chunk(q):
        def pass_on(r, carry):
            wait_recv(passing.at[q, r], ps_y.at[q, r])
            ahead, _, _ = ring(r)
            ysum[q, r, ahead] = (ysum[q, r, ahead].astype(F32) + passing[q, r].astype(F32)).astype(BF16)
            remote(ysum.at[q, r, ahead], yrecv.at[q, r, 1], ys_s, ys_r.at[q, r], (g, f, ahead * n_c + c)).start()
            return carry

        lax.fori_loop(0, NR, pass_on, 0)

    def combine(q):
        wait_recv(rrecv.at[q, pl.ds(0, (n_fs - 1) * cap), :], rt_r.at[q])
        dn = (((0,), (0,)), ((), ()))
        got = rrecv[q]
        out = lax.dot_general(share_hi[...], got, dn, preferred_element_type=F32)
        out = out + lax.dot_general(share_lo[...], got, dn, preferred_element_type=F32)
        mixed_out[:, q * wq : (q + 1) * wq] = out.astype(BF16)

    for q in range(NQ):
        if q == NQ - 1:
            pass_chunk(q - 1)
            finish(q - 2)

        @pl.when(z == t)
        def _(q=q):
            wait_recv(wg.at[pl.ds(0, all_but_one // NQ), :], d_r.at[q])

        @pl.when(z != t)
        def _(q=q):
            wait_recv(wg.at[pl.ds(0, wg.shape[0] // NQ), :], d_r.at[q])

        def for_sibling(r, carry, q=q):
            for yy in range(n_y):
                psend[q, r, yy] = partial(q, r, yy * n_c + (1 - c)).astype(BF16)
            remote(psend.at[q, r], precv.at[q, r], ps_s, ps_r.at[q, r], sibling).start()
            return carry

        if q + 2 < NQ:
            start_down(q + 2)
        lax.fori_loop(0, NR, for_sibling, 0)

        def for_own(r, carry, q=q):
            for yy in range(n_y):
                ysum[q, r, yy] = partial(q, r, yy * n_c + c).astype(BF16)
            return carry

        lax.fori_loop(0, NR, for_own, 0)

        def exchange(r, carry, q=q):
            wait_recv(precv.at[q, r], ps_r.at[q, r])
            for yy in range(n_y):
                ysum[q, r, yy] = (ysum[q, r, yy].astype(F32) + precv[q, r, yy].astype(F32)).astype(BF16)
            ahead, behind, far = ring(r)
            remote(ysum.at[q, r, far], passing.at[q, r], ys_s, ps_y.at[q, r], (g, f, ahead * n_c + c)).start()
            remote(ysum.at[q, r, behind], yrecv.at[q, r, 0], ys_s, ys_r.at[q, r], (g, f, behind * n_c + c)).start()
            return carry

        lax.fori_loop(0, NR, exchange, 0)
        if 0 < q < NQ - 1:
            pass_chunk(q - 1)
        if 1 < q < NQ - 1:
            finish(q - 2)
        if q > 2:
            combine(q - 3)
    finish(NQ - 2)
    pass_chunk(NQ - 1)
    finish(NQ - 1)
    for q in range(max(NQ - 3, 0), NQ):
        combine(q)

    wait_send(slots.at[pl.ds(0, (n_fs - 1) * cap), :], disp_s)
    wait_send(wg.at[pl.ds(0, all_but_one), :], w_s.at[0])
    wait_send(wu.at[pl.ds(0, all_but_one), :], w_s.at[1])

    @pl.when(z == t)
    def _():
        wait_send(wg.at[pl.ds(0, all_but_one), :], w_s.at[2])

    @pl.when(z != t)
    def _():
        wait_send(wg, w_s.at[2])

    wait_send(psend, ps_s)
    wait_send(ysum.at[:, :, pl.ds(0, n_y - 1)], ys_s)
    wait_send(rrecv.at[:, pl.ds(0, (n_fs - 1) * cap), :], rt_s)


def write_out(*refs):
    n = len(refs) // 2
    sem = refs[2 * n]
    copies = []
    for i, (src, dst) in enumerate(zip(refs[:n], refs[n : 2 * n])):
        parts = 4 if len(src.shape) == 3 else 1
        size = src.shape[-2] // parts
        for p in range(parts):
            rows = (slice(None),) * (len(src.shape) - 2) + (pl.ds(p * size, size),)
            copies.append(pltpu.make_async_copy(src.at[rows], dst.at[rows], sem.at[i, p]))
    for copy in copies:
        copy.start()
    for copy in copies:
        copy.wait()


def body(tokens, route_ids, route_logits, gain, gate_master, up_master, down_master, *, sizes):
    n_gr, n_zl, n_x, n_y, n_c = sizes
    experts, rows_g, ff = gate_master.shape
    rows_d, wide = down_master.shape[1:]
    n_tok, top = route_ids.shape
    cap = 2 * n_tok * top // experts
    n_fs, n_tp = n_zl * n_x, n_y * n_c
    n_rows = n_fs * cap
    d_model, hid = wide * n_tp, ff
    wq = wide // NQ
    vmem = lambda *shape, dtype=BF16: pltpu.VMEM(shape, dtype)
    dma = pltpu.SemaphoreType.DMA
    any_spec = pl.BlockSpec(memory_space=pl.ANY)
    vmem_spec = pl.BlockSpec(memory_space=pltpu.VMEM)
    results = pl.pallas_call(
        functools.partial(kernel, (n_gr, n_zl, n_x, n_y, n_c, cap)),
        out_shape=(
            pltpu.VMEM((1, d_model, ff), BF16),
            pltpu.VMEM((1, d_model, ff), BF16),
            pltpu.VMEM((1, hid, d_model), BF16),
            pltpu.VMEM((n_tok, wide), BF16),
        ),
        in_specs=[any_spec] * 7,
        out_specs=(vmem_spec,) * 4,
        scratch_shapes=[
            vmem(experts, rows_g, ff, dtype=F32),
            vmem(experts, rows_g, ff, dtype=F32),
            vmem(experts, rows_d, wide, dtype=F32),
            vmem(experts, rows_g, ff),
            vmem(experts, rows_g, ff),
            vmem(NQ, experts, rows_d, wq),
            vmem(n_rows, wide),
            vmem(n_rows, n_tok),
            vmem(n_rows, n_tok),
            vmem(n_tp, n_rows, wide),
            vmem(n_rows, hid, dtype=F32),
            vmem(n_rows, hid),
            vmem(n_tok, wide),
            vmem(top, n_tok, dtype=jnp.int32),
            vmem(top, n_tok, dtype=F32),
            vmem(1, rows_g, dtype=F32),
            vmem(NQ, NR, n_y, n_rows // NR, wq),
            vmem(NQ, NR, n_y, n_rows // NR, wq),
            vmem(NQ, NR, n_y, n_rows // NR, wq),
            vmem(NQ, NR, n_rows // NR, wq),
            vmem(NQ, NR, 2, n_rows // NR, wq),
            vmem(NQ, n_rows, wq),
            vmem(NQ, n_rows, wq),
            dma((7,)), dma, dma, dma((3,)), dma, dma, dma((NQ,)),
            dma, dma((n_y,)), dma, dma((n_y,)), dma, dma((NQ, NR)), dma, dma((NQ, NR)), dma((NQ, NR)), dma, dma((NQ,)),
        ],
        compiler_params=pltpu.CompilerParams(
            collective_id=0, has_side_effects=True, vmem_limit_bytes=50 * 1024 * 1024
        ),
    )(tokens, route_ids.T, route_logits.T, gain[None, :], gate_master, up_master, down_master)
    return pl.pallas_call(
        write_out,
        out_shape=tuple(jax.ShapeDtypeStruct(r.shape, r.dtype) for r in results),
        in_specs=[vmem_spec] * 4,
        out_specs=(any_spec,) * 4,
        scratch_shapes=[dma((4, 4))],
        compiler_params=pltpu.CompilerParams(vmem_limit_bytes=1024 * 1024),
    )(*(pltpu.with_memory_space_constraint(r, pltpu.VMEM) for r in results))


def solution(mesh):
    n_zl, n_x, n_c = 4, 4, 2
    sizes = (mesh.shape["gr"], n_zl, n_x, mesh.shape["tp"] // n_c, n_c)
    in_specs = (
        P(("gr", "fs"), "tp"),
        P(("gr", "fs"), None),
        P(("gr", "fs"), None),
        P(("gr", "fs")),
        P(None, ("gr", "fs"), "tp"),
        P(None, ("gr", "fs"), "tp"),
        P(None, ("gr", "fs"), "tp"),
    )
    out_specs = (
        P("fs", None, "tp"),
        P("fs", None, "tp"),
        P("fs", "tp", None),
        P(("gr", "fs"), "tp"),
    )
    return jax.shard_map(
        functools.partial(body, sizes=sizes), mesh=mesh, in_specs=in_specs, out_specs=out_specs, check_vma=False
    )
```
